256 devices in a mesh: rep: 2 (over z_hi), fs: 16 (over z_lo, x), tp: 8 (over y, core).
Axes of the slice: x: 4, y: 4, z: 8 (z_hi: 2, z_lo: 4; z = z_hi * 4 + z_lo), core: 2. Of those that a mesh axis runs over, the one named last changes fastest.
Arguments:
- tokens: bfloat16 [12288, 2048], P(('rep', 'fs'), 'tp'), may hold values from -6 to 6
- norm_gain: bfloat16 [2048], replicated, may hold values from 0.099609375 to 1.8984375
- w_gate: bfloat16 [2048, 5120], P('fs', 'tp'), may hold values from -0.125 to 0.125
- w_up: bfloat16 [2048, 5120], P('fs', 'tp'), may hold values from -0.125 to 0.125
- w_down: bfloat16 [5120, 2048], P('tp', 'fs'), may hold values from -0.078125 to 0.078125
- cotangent: bfloat16 [12288, 2048], P(('rep', 'fs'), 'tp'), may hold values from -6 to 6
Outputs:
- grad_tokens: bfloat16 [12288, 2048], P(('rep', 'fs'), 'tp')
- grad_gain: float32 [2048], P('tp')
- grad_gate: float32 [2048, 5120], P('fs', 'tp')
- grad_up: float32 [2048, 5120], P('fs', 'tp')
- grad_down: float32 [5120, 2048], P('tp', 'fs')
- gate_up_sq: float32 [2, 2048], P(None, 'fs')
- down_sq: float32 [5120], P('tp')
The draws below stay inside these ranges and needn't reach their ends.
All inputs are finite; a program needn't handle non-finite values.
Results may differ from the reference program's by a relative error of at most 0.018.
Values may be sent and summed in bfloat16 or wider, within the bound.
No kernel may reach another device: no remote copies, remote signals or barrier semaphores. Data moves between devices by JAX's collectives and lax.ppermute only.
A program may use at most 64 MiB of HBM per device.

```python
import jax
import jax.numpy as jnp
from jax import lax

D = 2048
FF = 5120
TOKENS = 12288


def raised(array, own_key, source, target, shards_of, factor):
    def block_of(position):
        return (jnp.arange(array.shape[position]) // (array.shape[position] // shards_of)).reshape((-1,) + (1,) * (array.ndim - 1 - position))

    first = jax.random.permutation(own_key, shards_of)[block_of(target)]
    far = (block_of(target) + shards_of // 2) % shards_of
    return jnp.where((block_of(source) == first) | (block_of(source) == far), factor * array, array)


def block_scale(rng, extent, pieces, smallest, top_value):
    factor_of = 1.0
    for position, shards_of in pieces:
        draws = jax.random.uniform(jax.random.fold_in(jax.random.fold_in(rng, 6), position), (shards_of,), jnp.float32, smallest / len(pieces), top_value / len(pieces))
        factor_of = factor_of * jnp.repeat(jnp.exp(draws), extent[position] // shards_of).reshape((-1,) + (1,) * (len(extent) - 1 - position))
    return factor_of


def scatter_about(stream_key, shape, scale, reach, split=(), held_as=jnp.bfloat16):
    gain = block_scale(stream_key, shape, split, -0.22, 0.18) if split else 1.0
    drawn = jax.random.normal(stream_key, shape, jnp.float32) * scale * gain
    return jnp.minimum(jnp.maximum(drawn, -reach), reach).astype(held_as)


def heavy_noise(own_key, extent, scale, limit, split, heavy, held_as=jnp.bfloat16):
    entries = scale * jax.random.normal(own_key, extent, jnp.float32)
    if split:
        entries = entries * block_scale(own_key, extent, split, -0.22, 0.18)
    return jnp.clip(raised(entries, jax.random.fold_in(own_key, 3), *heavy), -limit, limit).astype(held_as)


def setup_inputs(seed: int = 0) -> dict:
    splits = jax.random.split(jax.random.key(seed), 7)
    tokens = scatter_about(splits[0], (TOKENS, D), 1.0, 6.0, ((0, 32), (1, 8)))
    norm_gain = jnp.clip(1.0 + 0.18 * jax.random.normal(splits[1], (D,), jnp.float32), 0.099609375, 1.8984375).astype(jnp.bfloat16)
    w_gate = scatter_about(splits[2], (D, FF), D ** -0.5, 0.125, ((0, 16), (1, 8)))
    w_up = scatter_about(splits[3], (D, FF), D ** -0.5, 0.125, ((0, 16), (1, 8)))
    w_down = scatter_about(splits[4], (FF, D), FF ** -0.5, 0.078125, ((0, 8), (1, 16)))
    cotangent = heavy_noise(splits[5], (TOKENS, D), 1.0, 6.0, ((0, 32), (1, 8)), (0, 1, 32, 2.75))
    return {"tokens": tokens, "norm_gain": norm_gain, "w_gate": w_gate, "w_up": w_up, "w_down": w_down, "cotangent": cotangent}


def reference(tokens, norm_gain, w_gate, w_up, w_down, cotangent):
    wide_tokens = tokens.astype(jnp.float32)
    gain_f = norm_gain.astype(jnp.float32)
    inverse = jax.lax.rsqrt(lax.optimization_barrier(jnp.mean(wide_tokens * wide_tokens, axis=-1, keepdims=True)) + 1e-06)
    normed = (wide_tokens * inverse * gain_f).astype(jnp.bfloat16)
    gate = jnp.dot(normed, w_gate, preferred_element_type=jnp.float32)
    up_proj = jnp.dot(normed, w_up, preferred_element_type=jnp.float32)
    sigma = jax.nn.sigmoid(gate)
    active = gate * sigma
    hidden = (active * up_proj).astype(jnp.bfloat16)
    back = 0.5 * jnp.dot(cotangent, w_down.T, preferred_element_type=jnp.float32)
    d_up = (back * active).astype(jnp.bfloat16)
    d_gate = (back * up_proj * sigma * (1.0 + gate * (1.0 - sigma))).astype(jnp.bfloat16)
    d_normed = jnp.dot(d_gate, w_gate.T, preferred_element_type=jnp.float32) + jnp.dot(d_up, w_up.T, preferred_element_type=jnp.float32)
    grad_gain = lax.optimization_barrier(jnp.sum(d_normed * wide_tokens * inverse, axis=0))
    scaled_grad = d_normed * gain_f
    rowdot = lax.optimization_barrier(jnp.sum(scaled_grad * wide_tokens, axis=-1, keepdims=True))
    grad_tokens = (cotangent.astype(jnp.float32) + inverse * scaled_grad - wide_tokens * inverse ** 3 * rowdot / D).astype(jnp.bfloat16)
    grad_gate = jnp.einsum('td,tf->df', normed, d_gate, preferred_element_type=jnp.float32)
    grad_up = jnp.einsum('td,tf->df', normed, d_up, preferred_element_type=jnp.float32)
    grad_down = 0.5 * jnp.einsum('tf,td->fd', hidden, cotangent, preferred_element_type=jnp.float32)
    gate_up_sq = jnp.stack([lax.optimization_barrier(jnp.sum(grad_gate * grad_gate, axis=1)), lax.optimization_barrier(jnp.sum(grad_up * grad_up, axis=1))])
    down_sq = lax.optimization_barrier(jnp.sum(grad_down * grad_down, axis=1))
    return (grad_tokens, grad_gain, grad_gate, grad_up, grad_down, gate_up_sq, down_sq)
```

```python
import jax
import jax.numpy as jnp
from jax import lax
from jax.experimental import pallas as pl
from jax.experimental.pallas import tpu as pltpu
from jax.sharding import Mesh, PartitionSpec as P


F32 = jnp.float32
BF16 = jnp.bfloat16
TP = ("y", "core")
FS = ("zl", "x")
SPLIT = 1024


def over_x(a, shift):
    return lax.ppermute(a, "x", [(i, (i + shift) % 4) for i in range(4)])


def over_z(a, shift):
    return lax.ppermute(a, ("rep", "zl"), [(i, (i + shift) % 8) for i in range(8)])


def near_x(a):
    return [a, over_x(a, -1), over_x(a, -2), over_x(a, 1)]


def near_z(a):
    half = a.shape[0] // 2
    across = jnp.concatenate([over_z(a[:half], -2), over_z(a[half:], 2)], axis=0)
    return [a, over_z(a, -1), across, over_z(a, 1)]


def ring_gather(a, move):
    half = a.shape[0] // 2
    following, previous = move(a, -1), move(a, 1)
    return [a, following, move(following[:half], -1), move(previous[half:], 1), previous]


def added(*parts):
    total = parts[0].astype(F32)
    for p in parts[1:]:
        total = total + p.astype(F32)
    return total.astype(BF16)


def ring_reduce(blocks, move):
    half = blocks[0].shape[0] // 2
    ahead = move(jnp.concatenate([blocks[2][:half], blocks[1][half:]], axis=0), 1)
    behind = move(jnp.concatenate([blocks[2][half:], blocks[3][:half]], axis=0), -1)
    late_ahead = move(added(blocks[1][:half], ahead[:half]), 1)
    late_behind = move(added(blocks[3][half:], behind[:half]), -1)
    return jnp.concatenate(
        [
            added(blocks[0][:half], behind[half:], late_ahead),
            added(blocks[0][half:], ahead[half:], late_behind),
        ],
        axis=0,
    )


def to_each(a, axis):
    devices = lax.axis_size(axis)
    return lax.all_to_all(jnp.broadcast_to(a[None], (devices, *a.shape)), axis, 0, 0, tiled=True)


def prepare_kernel(order, both, gain, normed, dy, inverse):
    rows = 48

    def step(r, carry):
        at = pl.ds(pl.multiple_of(r * rows, rows), rows)
        squares = jnp.zeros((rows, 256), F32)
        for t in range(8):
            wide = both[t, at, :].astype(F32)
            squares = squares + wide * wide
        inv = lax.rsqrt(jnp.sum(squares, axis=-1, keepdims=True) / 2048 + 1e-06)
        inverse[at, :] = jnp.broadcast_to(inv, (rows, 128))
        below = pl.ds(pl.multiple_of(384 + r * rows, rows), rows)
        for j in range(16):
            t = order[j] // 2
            lanes = pl.ds(pl.multiple_of((order[j] % 2) * 128, 128), 128)
            wide = both[t, at, lanes].astype(F32)
            normed[at, j * 128 : (j + 1) * 128] = (wide * inv * gain[t, :, lanes]).astype(BF16)
            dy[at, j * 128 : (j + 1) * 128] = both[t, below, lanes]
        return carry

    lax.fori_loop(0, 384 // rows, step, 0)


def prepare(order, both, gain):
    whole = pl.BlockSpec(memory_space=pltpu.VMEM)
    return pl.pallas_call(
        prepare_kernel,
        out_shape=(
            jax.ShapeDtypeStruct((384, 2048), BF16),
            jax.ShapeDtypeStruct((384, 2048), BF16),
            jax.ShapeDtypeStruct((384, 128), F32),
        ),
        in_specs=[pl.BlockSpec(memory_space=pltpu.SMEM), whole, whole],
        out_specs=(whole, whole, whole),
        name="prepare",
    )(order, both, gain)


def restore_kernel(order, rotated, out):
    for j in range(16):
        t = order[j] // 2
        lanes = pl.ds(pl.multiple_of((order[j] % 2) * 128, 128), 128)
        out[t, :, lanes] = rotated[:, j * 128 : (j + 1) * 128]


def restore(order, rotated):
    whole = pl.BlockSpec(memory_space=pltpu.VMEM)
    return pl.pallas_call(
        restore_kernel,
        out_shape=jax.ShapeDtypeStruct((8, 384, 256), BF16),
        in_specs=[pl.BlockSpec(memory_space=pltpu.SMEM), whole],
        out_specs=whole,
        name="restore",
    )(order, rotated)


def contract_last(left, right):
    return lax.dot_general(left, right, (((1,), (1,)), ((), ())), preferred_element_type=F32)


def contract_first(left, right):
    return lax.dot_general(left, right, (((0,), (0,)), ((), ())), preferred_element_type=F32)


def on_device(tokens, norm_gain, w_gate, w_up, w_down, cotangent):
    zl, xi, tp = lax.axis_index("zl"), lax.axis_index("x"), lax.axis_index(TP)
    offsets = jnp.arange(16, dtype=jnp.int32)
    order = ((zl + offsets // 4) % 4) * 4 + (xi + offsets % 4) % 4
    gain_f = norm_gain.astype(F32)

    both = to_each(jnp.concatenate([tokens, cotangent], axis=0), TP)
    weights = jnp.concatenate([w_gate, w_up, w_down.T], axis=1)
    first = jnp.concatenate(near_x(weights[:, :SPLIT]), axis=0)
    second = jnp.concatenate(near_z(weights[:, SPLIT:]), axis=0)
    first = jnp.concatenate(ring_gather(first, over_z), axis=0)
    parts = ring_gather(second, over_x)
    parts = [parts[0], parts[1], jnp.concatenate(parts[2:4], axis=0), parts[4]]
    second = jnp.stack([p.reshape(4, 128, -1) for p in parts], axis=1).reshape(2048, -1)

    normed, dy, inv = prepare(order, both, gain_f.reshape(8, 1, 256))
    inverse = inv[:, :1]
    hid = w_gate.shape[1]
    rest = 2 * hid - SPLIT
    pre_first = jnp.dot(normed, first, preferred_element_type=F32)
    pre_rest = jnp.dot(normed, second[:, :rest], preferred_element_type=F32)
    gate = pre_first[:, :hid]
    up_proj = jnp.concatenate([pre_first[:, hid:], pre_rest], axis=1)
    sigma = jax.nn.sigmoid(gate)
    active = gate * sigma
    hidden = (active * up_proj).astype(BF16)
    back = 0.5 * jnp.dot(dy, second[:, rest:], preferred_element_type=F32)
    d_up = (back * active).astype(BF16)
    d_gate = (back * up_proj * sigma * (1.0 + gate * (1.0 - sigma))).astype(BF16)

    def blocks(left, right, scale=None):
        whole = contract_first(left, right)
        if scale is not None:
            whole = scale * whole
        return whole.astype(BF16).reshape(4, 4, 128, -1)

    def x_first(b):
        mine = ring_reduce([b[:, d] for d in range(4)], over_x)
        return ring_reduce([mine[d] for d in range(4)], over_z)

    def z_first(b):
        mine = ring_reduce([b[d] for d in range(4)], over_z)
        return ring_reduce([mine[d] for d in range(4)], over_x)

    def both_replicas(a):
        other = lax.ppermute(a, "rep", [(0, 1), (1, 0)])
        return a.astype(F32) + other.astype(F32)

    down_part = both_replicas(z_first(blocks(dy, hidden, 0.5)))
    grad_gate = both_replicas(x_first(blocks(normed, d_gate)))
    grad_up = both_replicas(x_first(blocks(normed, d_up)))

    d_pair = jnp.concatenate([d_gate, d_up], axis=1)
    partial_normed = contract_last(d_pair[:, :SPLIT], first) + contract_last(
        d_pair[:, SPLIT:], second[:, :rest]
    )
    arrived = lax.all_to_all(
        restore(order, partial_normed.astype(BF16)), TP, 0, 0, tiled=True
    )
    d_normed = jnp.sum(arrived.astype(F32), axis=0)
    local_width = d_normed.shape[1]
    local_gain = lax.dynamic_slice_in_dim(gain_f, tp * local_width, local_width, 0)
    local_tokens = tokens.astype(F32)
    scaled_grad = d_normed * local_gain
    rowdot = jnp.sum(to_each(jnp.sum(scaled_grad * local_tokens, axis=-1), TP), axis=0)
    grad_tokens = (
        cotangent.astype(F32)
        + inverse * scaled_grad
        - local_tokens * inverse**3 * rowdot[:, None] / 2048
    ).astype(BF16)
    grad_gain = jnp.sum(
        to_each(jnp.sum(d_normed * local_tokens * inverse, axis=0), ("rep", "zl", "x")), axis=0
    )
    grad_down = down_part.T
    gate_up_sq = jnp.sum(
        to_each(
            jnp.stack([jnp.sum(grad_gate * grad_gate, axis=1), jnp.sum(grad_up * grad_up, axis=1)]),
            TP,
        ),
        axis=0,
    )
    down_sq = jnp.sum(to_each(jnp.sum(down_part * down_part, axis=0), FS), axis=0)
    return (grad_tokens, grad_gain, grad_gate, grad_up, grad_down, gate_up_sq, down_sq)


def solution(mesh):
    fine = Mesh(mesh.devices.reshape(2, 4, 4, 4, 2), ("rep", "zl", "x", "y", "core"))
    rows = ("rep", "zl", "x")
    return jax.shard_map(
        on_device,
        mesh=fine,
        in_specs=(P(rows, TP), P(), P(FS, TP), P(FS, TP), P(TP, FS), P(rows, TP)),
        out_specs=(
            P(rows, TP),
            P(TP),
            P(FS, TP),
            P(FS, TP),
            P(TP, FS),
            P(None, FS),
            P(TP),
        ),
        check_vma=False,
    )
```

```python
import jax
import jax.numpy as jnp
from jax import lax
from jax.experimental import pallas as pl
from jax.experimental.pallas import tpu as pltpu
from jax.sharding import Mesh, PartitionSpec as P


F32 = jnp.float32
BF16 = jnp.bfloat16
TP = ("y", "core")
FS = ("zl", "x")
ROWS = 384
HID = 640
FIRST = 1024
SECOND = 896
REST = 2 * HID - FIRST


def over_x(a, shift):
    return lax.ppermute(a, "x", [(i, (i + shift) % 4) for i in range(4)])


def over_z(a, shift):
    return lax.ppermute(a, ("rep", "zl"), [(i, (i + shift) % 8) for i in range(8)])


def to_each(blocks, axis):
    return lax.all_to_all(blocks, axis, 0, 0, tiled=True)


def copies(a, axis):
    return to_each(jnp.broadcast_to(a[None], (lax.axis_size(axis), *a.shape)), axis)


def kernel(body, out, name, scalars=0, inputs=0, scratch=()):
    whole = pl.BlockSpec(memory_space=pltpu.VMEM)
    return pl.pallas_call(
        body,
        out_shape=[jax.ShapeDtypeStruct(s, d) for s, d in out],
        in_specs=[pl.BlockSpec(memory_space=pltpu.SMEM)] * scalars + [whole] * inputs,
        out_specs=[whole] * len(out),
        scratch_shapes=list(scratch),
        compiler_params=pltpu.CompilerParams(vmem_limit_bytes=60 << 20),
        name=name,
    )


def product(left, right):
    return jnp.dot(left, right, preferred_element_type=F32)


def product_last(left, right):
    return lax.dot_general(left, right, (((1,), (1,)), ((), ())), preferred_element_type=F32)


def pack_body(w_gate, w_up, w_down, first, second, upper, lower):
    first[:, :HID] = w_gate[...]
    first[:, HID:] = w_up[:, : FIRST - HID]
    turned = w_down[...].astype(F32).T.astype(BF16)
    for out, at in ((second, slice(0, 128)), (upper, slice(0, 64)), (lower, slice(64, 128))):
        out[:, :REST] = w_up[at, FIRST - HID :]
        out[:, REST:] = turned[at]


def prepare_body(order, both, gain, normed, dy, normed_t, dy_t, inverse):
    step = 128

    def rows_of(r, carry):
        at = pl.ds(pl.multiple_of(r * step, step), step)
        squares = jnp.zeros((step, 256), F32)
        for t in range(8):
            wide = both[t, at, :].astype(F32)
            squares = squares + wide * wide
        inv = lax.rsqrt(jnp.sum(squares, axis=-1, keepdims=True) / 2048 + 1e-06)
        inverse[at, :] = jnp.broadcast_to(inv, (step, 128))
        below = pl.ds(pl.multiple_of(ROWS + r * step, step), step)
        for j in range(16):
            t = order[j] // 2
            lanes = pl.ds(pl.multiple_of((order[j] % 2) * 128, 128), 128)
            scaled = both[t, at, lanes].astype(F32) * inv * gain[t, :, lanes]
            here = slice(j * 128, (j + 1) * 128)
            normed[at, here] = scaled.astype(BF16)
            normed_t[here, at] = scaled.T.astype(BF16)
            other = both[t, below, lanes]
            dy[at, here] = other
            dy_t[here, at] = other.astype(F32).T.astype(BF16)
        return carry

    lax.fori_loop(0, ROWS // step, rows_of, 0)


def forward_body(*refs):
    normed, dy, normed_t, dy_t = refs[:4]
    first, second = refs[4:12], refs[12:20]
    d_pair = refs[20]
    sent_first, sent_second = refs[21:26], refs[26:31]
    pre, rest, back, hidden = refs[31:]
    for i in range(8):
        term = product(normed[:, i * 256 : (i + 1) * 256], first[i][...])
        pre[...] = term if i == 0 else pre[...] + term
    for i in range(8):
        dx, half = i // 2, i % 2
        a = (8 * half + dx) * 128
        b = a + 512
        pair = jnp.concatenate([normed[:, a : a + 128], normed[:, b : b + 128]], axis=1)
        term = product(pair, second[i][:, :REST])
        rest[...] = term if i == 0 else rest[...] + term
        pair = jnp.concatenate([dy[:, a : a + 128], dy[:, b : b + 128]], axis=1)
        term = product(pair, second[i][:, REST:])
        back[...] = term if i == 0 else back[...] + term

    def gating(r, carry):
        at = pl.ds(pl.multiple_of(r * 32, 32), 32)
        gate = pre[at, :HID]
        up = jnp.concatenate([pre[at, HID:], rest[at, :]], axis=1)
        d_hidden = 0.5 * back[at, :]
        sigma = jax.nn.sigmoid(gate)
        active = gate * sigma
        hidden[at, :] = (active * up).astype(BF16)
        d_pair[at, HID:] = (d_hidden * active).astype(BF16)
        d_pair[at, :HID] = (d_hidden * up * sigma * (1.0 + gate * (1.0 - sigma))).astype(BF16)
        return carry

    lax.fori_loop(0, ROWS // 32, gating, 0)

    def place(sent, group, sub, columns, value):
        own, ahead, behind, late_ahead, late_behind = sent
        low = sub < 2
        if group == 0:
            own[sub, :, columns] = value
        elif group == 1 and low:
            late_ahead[sub, :, columns] = value
        elif group == 1 or (group == 2 and low):
            ahead[sub, :, columns] = value
        elif group == 2:
            behind[sub - 2, :, columns] = value
        elif low:
            behind[sub + 2, :, columns] = value
        else:
            late_behind[sub - 2, :, columns] = value

    for dz in range(4):
        at = slice(dz * 512, (dz + 1) * 512)
        grads = product(normed_t[at, :], d_pair[:, :FIRST]).astype(BF16)
        for dx in range(4):
            place(sent_first, dx, dz, slice(0, FIRST), grads[dx * 128 : (dx + 1) * 128])
        grads = product(normed_t[at, :], d_pair[:, FIRST:]).astype(BF16)
        for dx in range(4):
            place(sent_second, dz, dx, slice(0, REST), grads[dx * 128 : (dx + 1) * 128])
        grads = (0.5 * product(dy_t[at, :], hidden[...])).astype(BF16)
        for dx in range(4):
            place(sent_second, dz, dx, slice(REST, SECOND), grads[dx * 128 : (dx + 1) * 128])


def input_grad_body(order, d_pair, *refs):
    first, second, out = refs[:8], refs[8:16], refs[16]
    for i in range(8):
        dz, half = i // 2, i % 2
        total = product_last(d_pair[:, :FIRST], first[i][...])
        at = slice((dz % 2) * 128, (dz % 2) * 128 + 128)
        pair = [second[(2 * half + k) * 2 + dz // 2][at, :REST] for k in range(2)]
        total = total + product_last(d_pair[:, FIRST:], jnp.concatenate(pair, axis=0))
        for k in range(2):
            j = dz * 4 + half * 2 + k
            lanes = pl.ds(pl.multiple_of((order[j] % 2) * 128, 128), 128)
            out[order[j] // 2, :, lanes] = total[:, k * 128 : (k + 1) * 128].astype(BF16)


def late_body(kept_ahead, ahead, kept_behind, behind, to_ahead, to_behind):
    half = kept_ahead.shape[0]
    to_ahead[...] = (kept_ahead[...].astype(F32) + ahead[:half].astype(F32)).astype(BF16)
    to_behind[...] = (kept_behind[...].astype(F32) + behind[:half].astype(F32)).astype(BF16)


def turn_body(own, ahead, behind, late_ahead, late_behind, own2, to_ahead, to_behind, kept_ahead, kept_behind):
    def mine(sub):
        early, late, at = (behind, late_ahead, sub) if sub < 2 else (ahead, late_behind, sub - 2)
        total = own[sub].astype(F32) + early[at + 2].astype(F32) + late[at].astype(F32)
        return total.astype(BF16)

    own2[...] = mine(0)
    part = mine(1)
    kept_ahead[...] = part[:64]
    to_ahead[64:] = part[64:]
    part = mine(2)
    to_ahead[:64] = part[:64]
    to_behind[:64] = part[64:]
    part = mine(3)
    to_behind[64:] = part[:64]
    kept_behind[...] = part[64:]


def join_body(own, ahead, behind, late_ahead, late_behind, out):
    for at, early, late in ((slice(0, 64), behind, late_ahead), (slice(64, 128), ahead, late_behind)):
        total = own[at].astype(F32) + early[64:].astype(F32) + late[...].astype(F32)
        out[at] = total.astype(BF16)


def finish_body(first, first_other, second, second_other, gate, up, down, rows_sq, columns_sq):
    a = first[...].astype(F32) + first_other[...].astype(F32)
    b = second[...].astype(F32) + second_other[...].astype(F32)
    grad_gate = a[:, :HID]
    grad_up = jnp.concatenate([a[:, HID:], b[:, :REST]], axis=1)
    part = b[:, REST:]
    gate[...] = grad_gate
    up[...] = grad_up
    down[...] = part.T
    sums = []
    for g in (grad_gate, grad_up):
        s = g * g
        lanes = sum(s[:, k * 128 : (k + 1) * 128] for k in range(5))
        sums.append(jnp.sum(lanes.T, axis=0, keepdims=True))
    both = jnp.concatenate(sums, axis=0)
    for k in range(8):
        rows_sq[k] = both
    column = jnp.sum(part * part, axis=0, keepdims=True)
    for k in range(16):
        columns_sq[k] = column


def ring(sent, move):
    own, to_ahead, to_behind, kept_ahead, kept_behind = sent
    ahead, behind = move(to_ahead, 1), move(to_behind, -1)
    late = kernel(late_body, [(kept_ahead.shape, BF16)] * 2, "late", inputs=4)
    late_ahead, late_behind = late(kept_ahead, ahead, kept_behind, behind)
    return own, ahead, behind, move(late_ahead, 1), move(late_behind, -1)


def reduced(sent, moves, columns):
    out = [(128, columns)] * 3 + [(64, columns)] * 2
    turn = kernel(turn_body, [(s, BF16) for s in out], "turn", inputs=5)
    sent = turn(*ring(sent, moves[0]))
    join = kernel(join_body, [((128, columns), BF16)], "join", inputs=5)
    (mine,) = join(*ring(sent, moves[1]))
    return mine, lax.ppermute(mine, "rep", [(0, 1), (1, 0)])


def gathered(parts, move):
    a, b = jnp.concatenate(parts[:2], axis=0), jnp.concatenate(parts[2:], axis=0)
    next_a, next_b, last_a, last_b = move(a, -1), move(b, -1), move(a, 1), move(b, 1)
    return [a, b, next_a, next_b, move(next_a, -1), move(last_b, 1), last_a, last_b]


def on_device(tokens, norm_gain, w_gate, w_up, w_down, cotangent):
    zl, xi, tp = lax.axis_index("zl"), lax.axis_index("x"), lax.axis_index(TP)
    offsets = jnp.arange(16, dtype=jnp.int32)
    order = ((zl + offsets // 4) % 4) * 4 + (xi + offsets % 4) % 4
    gain_f = norm_gain.astype(F32)

    pack_out = [(128, FIRST), (128, SECOND), (64, SECOND), (64, SECOND)]
    pack = kernel(pack_body, [(s, BF16) for s in pack_out], "pack", inputs=3)
    first, second, upper, lower = pack(w_gate, w_up, w_down)
    first = gathered([first, over_x(first, -1), over_x(first, -2), over_x(first, 1)], over_z)
    far = jnp.concatenate([over_z(upper, -2), over_z(lower, 2)], axis=0)
    second = gathered([second, over_z(second, -1), far, over_z(second, 1)], over_x)

    both = copies(jnp.concatenate([tokens, cotangent], axis=0), TP)
    shape, turned = ((ROWS, 2048), BF16), ((2048, ROWS), BF16)
    prepare = kernel(
        prepare_body, [shape, shape, turned, turned, ((ROWS, 128), F32)], "prepare", 1, 2
    )
    normed, dy, normed_t, dy_t, inv = prepare(order, both, gain_f.reshape(8, 1, 256))
    inverse = inv[:, :1]

    out = [((ROWS, 2 * HID), BF16)]
    for columns in (FIRST, SECOND):
        out += [((n, 128, columns), BF16) for n in (4, 4, 4, 2, 2)]
    forward = kernel(
        forward_body,
        out,
        "forward",
        inputs=20,
        scratch=[
            pltpu.VMEM((ROWS, FIRST), F32),
            pltpu.VMEM((ROWS, REST), F32),
            pltpu.VMEM((ROWS, HID), F32),
            pltpu.VMEM((ROWS, HID), BF16),
        ],
    )
    d_pair, *sent = forward(normed, dy, normed_t, dy_t, *first, *second)
    mine_first = reduced(sent[:5], (over_x, over_z), FIRST)
    mine_second = reduced(sent[5:], (over_z, over_x), SECOND)

    input_grad = kernel(input_grad_body, [((8, ROWS, 256), BF16)], "input_grad", 1, 17)
    (shares,) = input_grad(order, d_pair, *first, *second)
    d_normed = jnp.sum(to_each(shares, TP).astype(F32), axis=0)
    local_width = d_normed.shape[1]
    local_gain = lax.dynamic_slice_in_dim(gain_f, tp * local_width, local_width, 0)
    local_tokens = tokens.astype(F32)
    scaled_grad = d_normed * local_gain
    rowdot = jnp.sum(copies(jnp.sum(scaled_grad * local_tokens, axis=-1), TP), axis=0)
    grad_tokens = (
        cotangent.astype(F32)
        + inverse * scaled_grad
        - local_tokens * inverse**3 * rowdot[:, None] / 2048
    ).astype(BF16)
    grad_gain = jnp.sum(
        copies(jnp.sum(d_normed * local_tokens * inverse, axis=0), ("rep", "zl", "x")), axis=0
    )

    wide = ((128, HID), F32)
    finish = kernel(
        finish_body,
        [wide, wide, ((HID, 128), F32), ((8, 2, 128), F32), ((16, 1, HID), F32)],
        "finish",
        inputs=4,
    )
    grad_gate, grad_up, grad_down, rows_sq, columns_sq = finish(*mine_first, *mine_second)
    gate_up_sq = jnp.sum(to_each(rows_sq, TP), axis=0)
    down_sq = jnp.sum(to_each(columns_sq, FS), axis=(0, 1))
    return (grad_tokens, grad_gain, grad_gate, grad_up, grad_down, gate_up_sq, down_sq)


def solution(mesh):
    fine = Mesh(mesh.devices.reshape(2, 4, 4, 4, 2), ("rep", "zl", "x", "y", "core"))
    rows = ("rep", "zl", "x")
    return jax.shard_map(
        on_device,
        mesh=fine,
        in_specs=(P(rows, TP), P(), P(FS, TP), P(FS, TP), P(TP, FS), P(rows, TP)),
        out_specs=(
            P(rows, TP),
            P(TP),
            P(FS, TP),
            P(FS, TP),
            P(TP, FS),
            P(None, FS),
            P(TP),
        ),
        check_vma=False,
    )
```

```python
import jax
import jax.numpy as jnp
from jax import lax
from jax.experimental import pallas as pl
from jax.experimental.pallas import tpu as pltpu
from jax.sharding import Mesh, PartitionSpec as P


F32 = jnp.float32
BF16 = jnp.bfloat16
TP = ("y", "core")
FS = ("zl", "x")
ROWS = 384
HID = 640
FIRST = 1024
SECOND = 896
REST = 2 * HID - FIRST


def over_x(a, shift):
    return lax.ppermute(a, "x", [(i, (i + shift) % 4) for i in range(4)])


def over_z(a, shift):
    return lax.ppermute(a, ("rep", "zl"), [(i, (i + shift) % 8) for i in range(8)])


def to_each(blocks, axis):
    return lax.all_to_all(blocks, axis, 0, 0, tiled=True)


def copies(a, axis):
    return to_each(jnp.broadcast_to(a[None], (lax.axis_size(axis), *a.shape)), axis)


def kernel(body, out, name, scalars=0, limit=8, scratch=(), far=False):
    whole = pl.BlockSpec(memory_space=pltpu.VMEM)

    def call(*args):
        near = [pltpu.with_memory_space_constraint(a, pltpu.VMEM) for a in args[scalars:]]
        return pl.pallas_call(
            body,
            out_shape=[jax.ShapeDtypeStruct(s, d) if far else pltpu.VMEM(s, d) for s, d in out],
            in_specs=[pl.BlockSpec(memory_space=pltpu.SMEM)] * scalars + [whole] * len(near),
            out_specs=[whole] * len(out),
            scratch_shapes=list(scratch),
            compiler_params=pltpu.CompilerParams(vmem_limit_bytes=limit << 20),
            name=name,
        )(*args[:scalars], *near)

    return call


def product(left, right):
    return jnp.dot(left, right, preferred_element_type=F32)


def product_last(left, right):
    return lax.dot_general(left, right, (((1,), (1,)), ((), ())), preferred_element_type=F32)


def pack_body(w_gate, w_up, w_down, first, second, upper, lower):
    first[:, :HID] = w_gate[...]
    first[:, HID:] = w_up[:, : FIRST - HID]
    turned = w_down[...].astype(F32).T.astype(BF16)
    for out, at in ((second, slice(0, 128)), (upper, slice(0, 64)), (lower, slice(64, 128))):
        out[:, :REST] = w_up[at, FIRST - HID :]
        out[:, REST:] = turned[at]


def prepare_body(order, both, gain, normed, dy, normed_t, dy_t, inverse):
    step = 128

    def rows_of(r, carry):
        at = pl.ds(pl.multiple_of(r * step, step), step)
        squares = jnp.zeros((step, 256), F32)
        for t in range(8):
            wide = both[t, at, :].astype(F32)
            squares = squares + wide * wide
        inv = lax.rsqrt(jnp.sum(squares, axis=-1, keepdims=True) / 2048 + 1e-06)
        inverse[at, :] = jnp.broadcast_to(inv, (step, 128))
        below = pl.ds(pl.multiple_of(ROWS + r * step, step), step)
        for j in range(16):
            t = order[j] // 2
            lanes = pl.ds(pl.multiple_of((order[j] % 2) * 128, 128), 128)
            scaled = both[t, at, lanes].astype(F32) * inv * gain[t, :, lanes]
            here = slice(j * 128, (j + 1) * 128)
            normed[at, here] = scaled.astype(BF16)
            normed_t[here, at] = scaled.T.astype(BF16)
            other = both[t, below, lanes]
            dy[at, here] = other
            dy_t[here, at] = other.astype(F32).T.astype(BF16)
        return carry

    lax.fori_loop(0, ROWS // step, rows_of, 0)


def forward_body(*refs):
    normed, dy, normed_t, dy_t = refs[:4]
    first, second = refs[4:12], refs[12:20]
    d_pair = refs[20]
    sent_first, sent_second = refs[21:26], refs[26:31]
    pre, rest, back, hidden = refs[31:]
    for i in range(8):
        term = product(normed[:, i * 256 : (i + 1) * 256], first[i][...])
        pre[...] = term if i == 0 else pre[...] + term
    for i in range(8):
        dx, half = i // 2, i % 2
        a = (8 * half + dx) * 128
        b = a + 512
        pair = jnp.concatenate([normed[:, a : a + 128], normed[:, b : b + 128]], axis=1)
        term = product(pair, second[i][:, :REST])
        rest[...] = term if i == 0 else rest[...] + term
        pair = jnp.concatenate([dy[:, a : a + 128], dy[:, b : b + 128]], axis=1)
        term = product(pair, second[i][:, REST:])
        back[...] = term if i == 0 else back[...] + term

    def gating(r, carry):
        at = pl.ds(pl.multiple_of(r * 32, 32), 32)
        gate = pre[at, :HID]
        up = jnp.concatenate([pre[at, HID:], rest[at, :]], axis=1)
        d_hidden = 0.5 * back[at, :]
        sigma = jax.nn.sigmoid(gate)
        active = gate * sigma
        hidden[at, :] = (active * up).astype(BF16)
        d_pair[at, HID:] = (d_hidden * active).astype(BF16)
        d_pair[at, :HID] = (d_hidden * up * sigma * (1.0 + gate * (1.0 - sigma))).astype(BF16)
        return carry

    lax.fori_loop(0, ROWS // 32, gating, 0)

    def place(sent, group, sub, columns, value):
        own, ahead, behind, late_ahead, late_behind = sent
        low = sub < 2
        if group == 0:
            own[sub, :, columns] = value
        elif group == 1 and low:
            late_ahead[sub, :, columns] = value
        elif group == 1 or (group == 2 and low):
            ahead[sub, :, columns] = value
        elif group == 2:
            behind[sub - 2, :, columns] = value
        elif low:
            behind[sub + 2, :, columns] = value
        else:
            late_behind[sub - 2, :, columns] = value

    for dz in range(4):
        at = slice(dz * 512, (dz + 1) * 512)
        grads = product(normed_t[at, :], d_pair[:, :FIRST]).astype(BF16)
        for dx in range(4):
            place(sent_first, dx, dz, slice(0, FIRST), grads[dx * 128 : (dx + 1) * 128])
        grads = product(normed_t[at, :], d_pair[:, FIRST:]).astype(BF16)
        for dx in range(4):
            place(sent_second, dz, dx, slice(0, REST), grads[dx * 128 : (dx + 1) * 128])
        grads = (0.5 * product(dy_t[at, :], hidden[...])).astype(BF16)
        for dx in range(4):
            place(sent_second, dz, dx, slice(REST, SECOND), grads[dx * 128 : (dx + 1) * 128])


def input_grad_body(order, d_pair, *refs):
    first, second, out = refs[:8], refs[8:16], refs[16]
    for i in range(8):
        dz, half = i // 2, i % 2
        total = product_last(d_pair[:, :FIRST], first[i][...])
        at = slice((dz % 2) * 128, (dz % 2) * 128 + 128)
        pair = [second[(2 * half + k) * 2 + dz // 2][at, :REST] for k in range(2)]
        total = total + product_last(d_pair[:, FIRST:], jnp.concatenate(pair, axis=0))
        for k in range(2):
            j = dz * 4 + half * 2 + k
            lanes = pl.ds(pl.multiple_of((order[j] % 2) * 128, 128), 128)
            out[order[j] // 2, :, lanes] = total[:, k * 128 : (k + 1) * 128].astype(BF16)


def late_body(kept_ahead, ahead, kept_behind, behind, to_ahead, to_behind):
    half = kept_ahead.shape[0]
    to_ahead[...] = (kept_ahead[...].astype(F32) + ahead[:half].astype(F32)).astype(BF16)
    to_behind[...] = (kept_behind[...].astype(F32) + behind[:half].astype(F32)).astype(BF16)


def turn_body(own, ahead, behind, late_ahead, late_behind, own2, to_ahead, to_behind, kept_ahead, kept_behind):
    def mine(sub):
        early, late, at = (behind, late_ahead, sub) if sub < 2 else (ahead, late_behind, sub - 2)
        total = own[sub].astype(F32) + early[at + 2].astype(F32) + late[at].astype(F32)
        return total.astype(BF16)

    own2[...] = mine(0)
    part = mine(1)
    kept_ahead[...] = part[:64]
    to_ahead[64:] = part[64:]
    part = mine(2)
    to_ahead[:64] = part[:64]
    to_behind[:64] = part[64:]
    part = mine(3)
    to_behind[64:] = part[:64]
    kept_behind[...] = part[64:]


def join_body(own, ahead, behind, late_ahead, late_behind, out):
    for at, early, late in ((slice(0, 64), behind, late_ahead), (slice(64, 128), ahead, late_behind)):
        total = own[at].astype(F32) + early[64:].astype(F32) + late[...].astype(F32)
        out[at] = total.astype(BF16)


def finish_body(first, first_other, second, second_other, gate, up, down, rows_sq, columns_sq):
    a = first[...].astype(F32) + first_other[...].astype(F32)
    b = second[...].astype(F32) + second_other[...].astype(F32)
    grad_gate = a[:, :HID]
    grad_up = jnp.concatenate([a[:, HID:], b[:, :REST]], axis=1)
    part = b[:, REST:]
    gate[...] = grad_gate
    up[...] = grad_up
    down[...] = part.T
    sums = []
    for g in (grad_gate, grad_up):
        s = g * g
        lanes = sum(s[:, k * 128 : (k + 1) * 128] for k in range(5))
        sums.append(jnp.sum(lanes.T, axis=0, keepdims=True))
    both = jnp.concatenate(sums, axis=0)
    for k in range(8):
        rows_sq[k] = both
    column = jnp.sum(part * part, axis=0, keepdims=True)
    for k in range(16):
        columns_sq[k] = column


def ring(sent, move):
    own, to_ahead, to_behind, kept_ahead, kept_behind = sent
    ahead, behind = move(to_ahead, 1), move(to_behind, -1)
    late = kernel(late_body, [(kept_ahead.shape, BF16)] * 2, "late")
    late_ahead, late_behind = late(kept_ahead, ahead, kept_behind, behind)
    return own, ahead, behind, move(late_ahead, 1), move(late_behind, -1)


def reduced(sent, moves, columns):
    out = [(128, columns)] * 3 + [(64, columns)] * 2
    turn = kernel(turn_body, [(s, BF16) for s in out], "turn")
    sent = turn(*ring(sent, moves[0]))
    join = kernel(join_body, [((128, columns), BF16)], "join")
    (mine,) = join(*ring(sent, moves[1]))
    return mine, lax.ppermute(mine, "rep", [(0, 1), (1, 0)])


def gathered(parts, move):
    a, b = jnp.concatenate(parts[:2], axis=0), jnp.concatenate(parts[2:], axis=0)
    next_a, next_b, last_a, last_b = move(a, -1), move(b, -1), move(a, 1), move(b, 1)
    return [a, b, next_a, next_b, move(next_a, -1), move(last_b, 1), last_a, last_b]


def on_device(tokens, norm_gain, w_gate, w_up, w_down, cotangent):
    zl, xi, tp = lax.axis_index("zl"), lax.axis_index("x"), lax.axis_index(TP)
    offsets = jnp.arange(16, dtype=jnp.int32)
    order = ((zl + offsets // 4) % 4) * 4 + (xi + offsets % 4) % 4
    gain_f = norm_gain.astype(F32)

    pack_out = [(128, FIRST), (128, SECOND), (64, SECOND), (64, SECOND)]
    pack = kernel(pack_body, [(s, BF16) for s in pack_out], "pack")
    first, second, upper, lower = pack(w_gate, w_up, w_down)
    first = gathered([first, over_x(first, -1), over_x(first, -2), over_x(first, 1)], over_z)
    far = jnp.concatenate([over_z(upper, -2), over_z(lower, 2)], axis=0)
    second = gathered([second, over_z(second, -1), far, over_z(second, 1)], over_x)

    both = copies(jnp.concatenate([tokens, cotangent], axis=0), TP)
    shape, turned = ((ROWS, 2048), BF16), ((2048, ROWS), BF16)
    prepare = kernel(
        prepare_body, [shape, shape, turned, turned, ((ROWS, 128), F32)], "prepare", 1, 16
    )
    normed, dy, normed_t, dy_t, inv = prepare(order, both, gain_f.reshape(8, 1, 256))
    inverse = inv[:, :1]

    out = [((ROWS, 2 * HID), BF16)]
    for columns in (FIRST, SECOND):
        out += [((n, 128, columns), BF16) for n in (4, 4, 4, 2, 2)]
    forward = kernel(
        forward_body,
        out,
        "forward",
        limit=26,
        scratch=[
            pltpu.VMEM((ROWS, FIRST), F32),
            pltpu.VMEM((ROWS, REST), F32),
            pltpu.VMEM((ROWS, HID), F32),
            pltpu.VMEM((ROWS, HID), BF16),
        ],
    )
    d_pair, *sent = forward(normed, dy, normed_t, dy_t, *first, *second)
    mine_first = reduced(sent[:5], (over_x, over_z), FIRST)
    mine_second = reduced(sent[5:], (over_z, over_x), SECOND)

    input_grad = kernel(input_grad_body, [((8, ROWS, 256), BF16)], "input_grad", 1, 24)
    (shares,) = input_grad(order, d_pair, *first, *second)
    d_normed = jnp.sum(to_each(shares, TP).astype(F32), axis=0)
    local_width = d_normed.shape[1]
    local_gain = lax.dynamic_slice_in_dim(gain_f, tp * local_width, local_width, 0)
    local_tokens = tokens.astype(F32)
    scaled_grad = d_normed * local_gain
    rowdot = jnp.sum(copies(jnp.sum(scaled_grad * local_tokens, axis=-1), TP), axis=0)
    grad_tokens = (
        cotangent.astype(F32)
        + inverse * scaled_grad
        - local_tokens * inverse**3 * rowdot[:, None] / 2048
    ).astype(BF16)
    grad_gain = jnp.sum(
        copies(jnp.sum(d_normed * local_tokens * inverse, axis=0), ("rep", "zl", "x")), axis=0
    )

    wide = ((128, HID), F32)
    finish = kernel(
        finish_body,
        [wide, wide, ((HID, 128), F32), ((8, 2, 128), F32), ((16, 1, HID), F32)],
        "finish",
        far=True,
    )
    grad_gate, grad_up, grad_down, rows_sq, columns_sq = finish(*mine_first, *mine_second)
    gate_up_sq = jnp.sum(to_each(rows_sq, TP), axis=0)
    down_sq = jnp.sum(to_each(columns_sq, FS), axis=(0, 1))
    return (grad_tokens, grad_gain, grad_gate, grad_up, grad_down, gate_up_sq, down_sq)


def solution(mesh):
    fine = Mesh(mesh.devices.reshape(2, 4, 4, 4, 2), ("rep", "zl", "x", "y", "core"))
    rows = ("rep", "zl", "x")
    return jax.shard_map(
        on_device,
        mesh=fine,
        in_specs=(P(rows, TP), P(), P(FS, TP), P(FS, TP), P(TP, FS), P(rows, TP)),
        out_specs=(
            P(rows, TP),
            P(TP),
            P(FS, TP),
            P(FS, TP),
            P(TP, FS),
            P(None, FS),
            P(TP),
        ),
        check_vma=False,
    )
```

```python
import jax
import jax.numpy as jnp
from jax import lax
from jax.experimental import pallas as pl
from jax.experimental.pallas import tpu as pltpu
from jax.sharding import Mesh, PartitionSpec as P


F32 = jnp.float32
BF16 = jnp.bfloat16
TP = ("y", "core")
SWAP = [(0, 1), (1, 0)]
FS = ("zl", "x")
ROWS = 384
HID = 640
FIRST = 1024
SECOND = 896
REST = 2 * HID - FIRST


def over_x(a, shift):
    return lax.ppermute(a, "x", [(i, (i + shift) % 4) for i in range(4)])


def over_z(a, shift):
    return lax.ppermute(a, ("rep", "zl"), [(i, (i + shift) % 8) for i in range(8)])


def to_each(blocks, axis):
    return lax.all_to_all(blocks, axis, 0, 0, tiled=True)


def copies(a, axis):
    return to_each(jnp.broadcast_to(a[None], (lax.axis_size(axis), *a.shape)), axis)


def kernel(body, out, name, scalars=0, limit=8, scratch=(), far=False):
    whole = pl.BlockSpec(memory_space=pltpu.VMEM)

    def call(*args):
        near = [pltpu.with_memory_space_constraint(a, pltpu.VMEM) for a in args[scalars:]]
        return pl.pallas_call(
            body,
            out_shape=[jax.ShapeDtypeStruct(s, d) if far else pltpu.VMEM(s, d) for s, d in out],
            in_specs=[pl.BlockSpec(memory_space=pltpu.SMEM)] * scalars + [whole] * len(near),
            out_specs=[whole] * len(out),
            scratch_shapes=list(scratch),
            compiler_params=pltpu.CompilerParams(vmem_limit_bytes=limit << 20),
            name=name,
        )(*args[:scalars], *near)

    return call


def product(left, right):
    return jnp.dot(left, right, preferred_element_type=F32)


def product_last(left, right):
    return lax.dot_general(left, right, (((1,), (1,)), ((), ())), preferred_element_type=F32)


def pack_body(w_gate, w_up, w_down, first, second, upper, lower):
    first[:, :HID] = w_gate[...]
    first[:, HID:] = w_up[:, : FIRST - HID]
    turned = w_down[...].astype(F32).T.astype(BF16)
    for out, at in ((second, slice(0, 128)), (upper, slice(0, 64)), (lower, slice(64, 128))):
        out[:, :REST] = w_up[at, FIRST - HID :]
        out[:, REST:] = turned[at]


def prepare_body(order, both, gain, normed, dy, normed_t, dy_t, inverse):
    step = 128

    def rows_of(r, carry):
        at = pl.ds(pl.multiple_of(r * step, step), step)
        squares = jnp.zeros((step, 256), F32)
        for t in range(8):
            wide = both[t, at, :].astype(F32)
            squares = squares + wide * wide
        inv = lax.rsqrt(jnp.sum(squares, axis=-1, keepdims=True) / 2048 + 1e-06)
        inverse[at, :] = jnp.broadcast_to(inv, (step, 128))
        below = pl.ds(pl.multiple_of(ROWS + r * step, step), step)
        for j in range(16):
            t = order[j] // 2
            lanes = pl.ds(pl.multiple_of((order[j] % 2) * 128, 128), 128)
            scaled = both[t, at, lanes].astype(F32) * inv * gain[t, :, lanes]
            here = slice(j * 128, (j + 1) * 128)
            normed[at, here] = scaled.astype(BF16)
            normed_t[here, at] = scaled.T.astype(BF16)
            other = both[t, below, lanes]
            dy[at, here] = other
            dy_t[here, at] = other.astype(F32).T.astype(BF16)
        return carry

    lax.fori_loop(0, ROWS // step, rows_of, 0)


def forward_body(*refs):
    normed, dy, normed_t, dy_t = refs[:4]
    first, second = refs[4:12], refs[12:20]
    d_pair = refs[20]
    sent_first, sent_second = refs[21:26], refs[26:31]
    pre, rest, back, hidden = refs[31:]
    for i in range(8):
        term = product(normed[:, i * 256 : (i + 1) * 256], first[i][...])
        pre[...] = term if i == 0 else pre[...] + term
    for i in range(8):
        dx, half = i // 2, i % 2
        a = (8 * half + dx) * 128
        b = a + 512
        pair = jnp.concatenate([normed[:, a : a + 128], normed[:, b : b + 128]], axis=1)
        term = product(pair, second[i][:, :REST])
        rest[...] = term if i == 0 else rest[...] + term
        pair = jnp.concatenate([dy[:, a : a + 128], dy[:, b : b + 128]], axis=1)
        term = product(pair, second[i][:, REST:])
        back[...] = term if i == 0 else back[...] + term

    def gating(r, carry):
        at = pl.ds(pl.multiple_of(r * 32, 32), 32)
        gate = pre[at, :HID]
        up = jnp.concatenate([pre[at, HID:], rest[at, :]], axis=1)
        d_hidden = 0.5 * back[at, :]
        sigma = jax.nn.sigmoid(gate)
        active = gate * sigma
        hidden[at, :] = (active * up).astype(BF16)
        d_pair[at, HID:] = (d_hidden * active).astype(BF16)
        d_pair[at, :HID] = (d_hidden * up * sigma * (1.0 + gate * (1.0 - sigma))).astype(BF16)
        return carry

    lax.fori_loop(0, ROWS // 32, gating, 0)

    def place(sent, group, sub, columns, value):
        own, ahead, behind, late_ahead, late_behind = sent
        low = sub < 2
        if group == 0:
            own[sub, :, columns] = value
        elif group == 1 and low:
            late_ahead[sub, :, columns] = value
        elif group == 1 or (group == 2 and low):
            ahead[sub, :, columns] = value
        elif group == 2:
            behind[sub - 2, :, columns] = value
        elif low:
            behind[sub + 2, :, columns] = value
        else:
            late_behind[sub - 2, :, columns] = value

    for dz in range(4):
        at = slice(dz * 512, (dz + 1) * 512)
        grads = product(normed_t[at, :], d_pair[:, :FIRST]).astype(BF16)
        for dx in range(4):
            place(sent_first, dx, dz, slice(0, FIRST), grads[dx * 128 : (dx + 1) * 128])
        grads = product(normed_t[at, :], d_pair[:, FIRST:]).astype(BF16)
        for dx in range(4):
            place(sent_second, dz, dx, slice(0, REST), grads[dx * 128 : (dx + 1) * 128])
        grads = (0.5 * product(dy_t[at, :], hidden[...])).astype(BF16)
        for dx in range(4):
            place(sent_second, dz, dx, slice(REST, SECOND), grads[dx * 128 : (dx + 1) * 128])


def input_grad_body(order, d_pair, *refs):
    first, second, out = refs[:8], refs[8:16], refs[16]
    for i in range(8):
        dz, half = i // 2, i % 2
        total = product_last(d_pair[:, :FIRST], first[i][...])
        at = slice((dz % 2) * 128, (dz % 2) * 128 + 128)
        pair = [second[(2 * half + k) * 2 + dz // 2][at, :REST] for k in range(2)]
        total = total + product_last(d_pair[:, FIRST:], jnp.concatenate(pair, axis=0))
        for k in range(2):
            j = dz * 4 + half * 2 + k
            lanes = pl.ds(pl.multiple_of((order[j] % 2) * 128, 128), 128)
            out[order[j] // 2, :, lanes] = total[:, k * 128 : (k + 1) * 128].astype(BF16)


def late_body(kept_ahead, ahead, kept_behind, behind, to_ahead, to_behind):
    half = kept_ahead.shape[0]
    to_ahead[...] = (kept_ahead[...].astype(F32) + ahead[:half].astype(F32)).astype(BF16)
    to_behind[...] = (kept_behind[...].astype(F32) + behind[:half].astype(F32)).astype(BF16)


def turn_body(own, ahead, behind, late_ahead, late_behind, *mine):
    for sub in range(4):
        early, late, at = (behind, late_ahead, sub) if sub < 2 else (ahead, late_behind, sub - 2)
        total = own[sub].astype(F32) + early[at + 2].astype(F32) + late[at].astype(F32)
        total = total.astype(BF16)
        if sub == 2 and len(mine) == 5:
            mine[2][...] = total[:64]
            mine[4][...] = total[64:]
        else:
            mine[sub][...] = total


def join_body(own, ahead, across, behind, *rest):
    far = across[...] if len(rest) == 1 else jnp.concatenate([across[...], rest[0][...]], axis=0)
    pair = own[...].astype(F32) + far.astype(F32)
    rest[-1][...] = (pair + (ahead[...].astype(F32) + behind[...].astype(F32))).astype(BF16)


def finish_second_body(mine, other, gain_sum, up_rest, up_sq, down, columns):
    b = mine[...].astype(F32) + other[...].astype(F32)
    rest, part = b[:, :REST], b[:, REST:]
    up_rest[...] = rest
    s = rest * rest
    up_sq[...] = s[:, :128] + s[:, 128:]
    down[...] = part.T
    column = jnp.sum(part * part, axis=0, keepdims=True)
    for k in range(16):
        columns[k, :, :HID] = column
        columns[k, :, HID:] = gain_sum[...]


def finish_first_body(mine, other, up_rest, up_sq, gate, up, rows_sq):
    a = mine[...].astype(F32) + other[...].astype(F32)
    gate[...] = a[:, :HID]
    up[:, : HID - REST] = a[:, HID:]
    up[:, HID - REST :] = up_rest[...]
    s = a * a
    gate_lanes = sum(s[:, k * 128 : (k + 1) * 128] for k in range(5))
    up_lanes = up_sq[...] + sum(s[:, k * 128 : (k + 1) * 128] for k in range(5, 8))
    sums = [jnp.sum(lanes.T, axis=0, keepdims=True) for lanes in (gate_lanes, up_lanes)]
    both = jnp.concatenate(sums, axis=0)
    for k in range(8):
        rows_sq[k] = both


def ring(sent, move):
    own, to_ahead, to_behind, kept_ahead, kept_behind = sent
    ahead, behind = move(to_ahead, 1), move(to_behind, -1)
    late = kernel(late_body, [(kept_ahead.shape, BF16)] * 2, "late")
    late_ahead, late_behind = late(kept_ahead, ahead, kept_behind, behind)
    return own, ahead, behind, move(late_ahead, 1), move(late_behind, -1)


def reduced(sent, moves, columns):
    halves = moves[1] is over_z
    out = [(128, columns)] * 2 + [(64 if halves else 128, columns), (128, columns)]
    out += [(64, columns)] * halves
    turn = kernel(turn_body, [(s, BF16) for s in out], "turn")
    own, one, two, three, *more = turn(*ring(sent, moves[0]))
    move = moves[1]
    terms = [own, move(one, 1), move(two, 2), move(three, -1)] + [move(m, -2) for m in more]
    (mine,) = kernel(join_body, [((128, columns), BF16)], "join")(*terms)
    return mine, lax.ppermute(mine, "rep", SWAP)


def gathered(parts, move):
    a, b = jnp.concatenate(parts[:2], axis=0), jnp.concatenate(parts[2:], axis=0)
    next_a, next_b, last_a, last_b = move(a, -1), move(b, -1), move(a, 1), move(b, 1)
    return [a, b, next_a, next_b, move(next_a, -1), move(last_b, 1), last_a, last_b]


def on_device(tokens, norm_gain, w_gate, w_up, w_down, cotangent):
    zl, xi, tp = lax.axis_index("zl"), lax.axis_index("x"), lax.axis_index(TP)
    offsets = jnp.arange(16, dtype=jnp.int32)
    order = ((zl + offsets // 4) % 4) * 4 + (xi + offsets % 4) % 4
    gain_f = norm_gain.astype(F32)

    pack_out = [(128, FIRST), (128, SECOND), (64, SECOND), (64, SECOND)]
    pack = kernel(pack_body, [(s, BF16) for s in pack_out], "pack")
    first, second, upper, lower = pack(w_gate, w_up, w_down)
    first = gathered([first, over_x(first, -1), over_x(first, -2), over_x(first, 1)], over_z)
    far = jnp.concatenate([over_z(upper, -2), over_z(lower, 2)], axis=0)
    second = gathered([second, over_z(second, -1), far, over_z(second, 1)], over_x)

    both = copies(jnp.concatenate([tokens, cotangent], axis=0), TP)
    shape, turned = ((ROWS, 2048), BF16), ((2048, ROWS), BF16)
    prepare = kernel(
        prepare_body, [shape, shape, turned, turned, ((ROWS, 128), F32)], "prepare", 1, 16
    )
    normed, dy, normed_t, dy_t, inv = prepare(order, both, gain_f.reshape(8, 1, 256))
    inverse = inv[:, :1]

    out = [((ROWS, 2 * HID), BF16)]
    for columns in (FIRST, SECOND):
        out += [((n, 128, columns), BF16) for n in (4, 4, 4, 2, 2)]
    forward = kernel(
        forward_body,
        out,
        "forward",
        limit=26,
        scratch=[
            pltpu.VMEM((ROWS, FIRST), F32),
            pltpu.VMEM((ROWS, REST), F32),
            pltpu.VMEM((ROWS, HID), F32),
            pltpu.VMEM((ROWS, HID), BF16),
        ],
    )
    d_pair, *sent = forward(normed, dy, normed_t, dy_t, *first, *second)
    mine_first = reduced(sent[:5], (over_x, over_z), FIRST)
    mine_second = reduced(sent[5:], (over_z, over_x), SECOND)

    input_grad = kernel(input_grad_body, [((8, ROWS, 256), BF16)], "input_grad", 1, 24)
    (shares,) = input_grad(order, d_pair, *first, *second)
    d_normed = jnp.sum(to_each(shares, TP).astype(F32), axis=0)
    local_width = d_normed.shape[1]
    local_gain = lax.dynamic_slice_in_dim(gain_f, tp * local_width, local_width, 0)
    local_tokens = tokens.astype(F32)
    scaled_grad = d_normed * local_gain
    rowdot = jnp.sum(copies(jnp.sum(scaled_grad * local_tokens, axis=-1), TP), axis=0)
    grad_tokens = (
        cotangent.astype(F32)
        + inverse * scaled_grad
        - local_tokens * inverse**3 * rowdot[:, None] / 2048
    ).astype(BF16)
    gain_part = jnp.sum(d_normed * local_tokens * inverse, axis=0, keepdims=True)
    gain_part = gain_part + lax.ppermute(gain_part, "rep", SWAP)

    square, wide = ((128, 128), F32), ((128, HID), F32)
    finish_second = kernel(
        finish_second_body,
        [((128, REST), F32), square, ((HID, 128), F32), ((16, 1, HID + 256), F32)],
        "finish_second",
        far=True,
    )
    up_rest, up_sq, grad_down, columns = finish_second(*mine_second, gain_part)
    sums = jnp.sum(to_each(columns, FS), axis=0)[0]
    down_sq, grad_gain = sums[:HID], sums[HID:]
    finish_first = kernel(
        finish_first_body, [wide, wide, ((8, 2, 128), F32)], "finish_first", far=True
    )
    grad_gate, grad_up, rows_sq = finish_first(*mine_first, up_rest, up_sq)
    gate_up_sq = jnp.sum(to_each(rows_sq, TP), axis=0)
    return (grad_tokens, grad_gain, grad_gate, grad_up, grad_down, gate_up_sq, down_sq)


def solution(mesh):
    fine = Mesh(mesh.devices.reshape(2, 4, 4, 4, 2), ("rep", "zl", "x", "y", "core"))
    rows = ("rep", "zl", "x")
    return jax.shard_map(
        on_device,
        mesh=fine,
        in_specs=(P(rows, TP), P(), P(FS, TP), P(FS, TP), P(TP, FS), P(rows, TP)),
        out_specs=(
            P(rows, TP),
            P(TP),
            P(FS, TP),
            P(FS, TP),
            P(TP, FS),
            P(None, FS),
            P(TP),
        ),
        check_vma=False,
    )
```

```python
import jax
import jax.numpy as jnp
from jax import lax
from jax.experimental import pallas as pl
from jax.experimental.pallas import tpu as pltpu
from jax.sharding import Mesh, PartitionSpec as P


F32 = jnp.float32
BF16 = jnp.bfloat16
TP = ("y", "core")
SWAP = [(0, 1), (1, 0)]
FS = ("zl", "x")
ROWS = 384
HID = 640
FIRST = 896
SECOND = 1024
REST = 2 * HID - FIRST


def over_x(a, shift):
    return lax.ppermute(a, "x", [(i, (i + shift) % 4) for i in range(4)])


def over_z(a, shift):
    return lax.ppermute(a, ("rep", "zl"), [(i, (i + shift) % 8) for i in range(8)])


def to_each(blocks, axis):
    return lax.all_to_all(blocks, axis, 0, 0, tiled=True)


def copies(a, axis):
    return to_each(jnp.broadcast_to(a[None], (lax.axis_size(axis), *a.shape)), axis)


def kernel(body, out, scalars=0, limit=8, scratch=(), far=()):
    whole = pl.BlockSpec(memory_space=pltpu.VMEM)

    def call(*args):
        near = [pltpu.with_memory_space_constraint(a, pltpu.VMEM) for a in args[scalars:]]
        return pl.pallas_call(
            body,
            out_shape=[
                pltpu.HBM(s, d) if i in far else pltpu.VMEM(s, d)
                for i, (s, d) in enumerate(out)
            ],
            in_specs=[pl.BlockSpec(memory_space=pltpu.SMEM)] * scalars + [whole] * len(near),
            out_specs=[whole] * len(out),
            scratch_shapes=list(scratch),
            compiler_params=pltpu.CompilerParams(vmem_limit_bytes=limit << 20),
        )(*args[:scalars], *near)

    return call


def product(left, right):
    return jnp.dot(left, right, preferred_element_type=F32)


def product_last(left, right):
    return lax.dot_general(left, right, (((1,), (1,)), ((), ())), preferred_element_type=F32)


def pack_body(w_gate, w_up, w_down, first, second, upper, lower):
    first[:, :HID] = w_gate[...]
    first[:, HID:] = w_up[:, : FIRST - HID]
    turned = w_down[...].astype(F32).T.astype(BF16)
    for out, at in ((second, slice(0, 128)), (upper, slice(0, 64)), (lower, slice(64, 128))):
        out[:, :REST] = w_up[at, FIRST - HID :]
        out[:, REST:] = turned[at]


def prepare_body(order, both, gain, normed, dy, normed_t, dy_t, inverse):
    step = 128

    def rows_of(r, carry):
        at = pl.ds(pl.multiple_of(r * step, step), step)
        squares = jnp.zeros((step, 256), F32)
        for t in range(8):
            wide = both[t, at, :].astype(F32)
            squares = squares + wide * wide
        inv = lax.rsqrt(jnp.sum(squares, axis=-1, keepdims=True) / 2048 + 1e-06)
        inverse[at, :] = jnp.broadcast_to(inv, (step, 128))
        below = pl.ds(pl.multiple_of(ROWS + r * step, step), step)
        for j in range(16):
            t = order[j] // 2
            lanes = pl.ds(pl.multiple_of((order[j] % 2) * 128, 128), 128)
            scaled = both[t, at, lanes].astype(F32) * inv * gain[t, :, lanes]
            here = slice(j * 128, (j + 1) * 128)
            normed[at, here] = scaled.astype(BF16)
            normed_t[here, at] = scaled.T.astype(BF16)
            other = both[t, below, lanes]
            dy[at, here] = other
            dy_t[here, at] = other.astype(F32).T.astype(BF16)
        return carry

    lax.fori_loop(0, ROWS // step, rows_of, 0)


def forward_body(*refs):
    normed, dy, normed_t, dy_t = refs[:4]
    first, second = refs[4:12], refs[12:20]
    d_pair = refs[20]
    sent_first, sent_second = refs[21:26], refs[26:31]
    pre, rest, back, hidden = refs[31:]
    for i in range(8):
        term = product(normed[:, i * 256 : (i + 1) * 256], first[i][...])
        pre[...] = term if i == 0 else pre[...] + term
    for i in range(8):
        dx, half = i // 2, i % 2
        a = (8 * half + dx) * 128
        b = a + 512
        pair = jnp.concatenate([normed[:, a : a + 128], normed[:, b : b + 128]], axis=1)
        term = product(pair, second[i][:, :REST])
        rest[...] = term if i == 0 else rest[...] + term
        pair = jnp.concatenate([dy[:, a : a + 128], dy[:, b : b + 128]], axis=1)
        term = product(pair, second[i][:, REST:])
        back[...] = term if i == 0 else back[...] + term

    def gating(r, carry):
        at = pl.ds(pl.multiple_of(r * 32, 32), 32)
        gate = pre[at, :HID]
        up = jnp.concatenate([pre[at, HID:], rest[at, :]], axis=1)
        d_hidden = 0.5 * back[at, :]
        sigma = jax.nn.sigmoid(gate)
        active = gate * sigma
        hidden[at, :] = (active * up).astype(BF16)
        d_pair[at, HID:] = (d_hidden * active).astype(BF16)
        d_pair[at, :HID] = (d_hidden * up * sigma * (1.0 + gate * (1.0 - sigma))).astype(BF16)
        return carry

    lax.fori_loop(0, ROWS // 32, gating, 0)

    def place(sent, group, sub, columns, value):
        own, ahead, behind, late_ahead, late_behind = sent
        low = sub < 2
        if group == 0:
            own[sub, :, columns] = value
        elif group == 1 and low:
            late_ahead[sub, :, columns] = value
        elif group == 1 or (group == 2 and low):
            ahead[sub, :, columns] = value
        elif group == 2:
            behind[sub - 2, :, columns] = value
        elif low:
            behind[sub + 2, :, columns] = value
        else:
            late_behind[sub - 2, :, columns] = value

    for dz in range(4):
        at = slice(dz * 512, (dz + 1) * 512)
        grads = product(normed_t[at, :], d_pair[:, :FIRST]).astype(BF16)
        for dx in range(4):
            place(sent_first, dx, dz, slice(0, FIRST), grads[dx * 128 : (dx + 1) * 128])
        grads = product(normed_t[at, :], d_pair[:, FIRST:]).astype(BF16)
        for dx in range(4):
            place(sent_second, dz, dx, slice(0, REST), grads[dx * 128 : (dx + 1) * 128])
        grads = (0.5 * product(dy_t[at, :], hidden[...])).astype(BF16)
        for dx in range(4):
            place(sent_second, dz, dx, slice(REST, SECOND), grads[dx * 128 : (dx + 1) * 128])


def input_grad_body(order, d_pair, *refs):
    first, second, out = refs[:8], refs[8:16], refs[16]
    for i in range(8):
        dz, half = i // 2, i % 2
        total = product_last(d_pair[:, :FIRST], first[i][...])
        at = slice((dz % 2) * 128, (dz % 2) * 128 + 128)
        pair = [second[(2 * half + k) * 2 + dz // 2][at, :REST] for k in range(2)]
        total = total + product_last(d_pair[:, FIRST:], jnp.concatenate(pair, axis=0))
        for k in range(2):
            j = dz * 4 + half * 2 + k
            lanes = pl.ds(pl.multiple_of((order[j] % 2) * 128, 128), 128)
            out[order[j] // 2, :, lanes] = total[:, k * 128 : (k + 1) * 128].astype(BF16)


def late_body(kept_ahead, ahead, kept_behind, behind, to_ahead, to_behind):
    half = kept_ahead.shape[0]
    to_ahead[...] = (kept_ahead[...].astype(F32) + ahead[:half].astype(F32)).astype(BF16)
    to_behind[...] = (kept_behind[...].astype(F32) + behind[:half].astype(F32)).astype(BF16)


def turn_body(own, ahead, behind, late_ahead, late_behind, *mine):
    for sub in range(4):
        early, late, at = (behind, late_ahead, sub) if sub < 2 else (ahead, late_behind, sub - 2)
        total = own[sub].astype(F32) + early[at + 2].astype(F32) + late[at].astype(F32)
        total = total.astype(BF16)
        if sub == 2 and len(mine) == 5:
            mine[2][...] = total[:64]
            mine[4][...] = total[64:]
        else:
            mine[sub][...] = total


def join_body(own, ahead, across, behind, *rest):
    far = across[...] if len(rest) == 1 else jnp.concatenate([across[...], rest[0][...]], axis=0)
    pair = own[...].astype(F32) + far.astype(F32)
    rest[-1][...] = (pair + (ahead[...].astype(F32) + behind[...].astype(F32))).astype(BF16)


def finish_second_body(mine, other, gain_sum, up_rest, up_sq, down, columns):
    b = mine[...].astype(F32) + other[...].astype(F32)
    rest, part = b[:, :REST], b[:, REST:]
    up_rest[...] = rest
    s = rest * rest
    up_sq[...] = sum(s[:, k * 128 : (k + 1) * 128] for k in range(REST // 128))
    down[...] = part.T
    column = jnp.sum(part * part, axis=0, keepdims=True)
    columns[:, :HID] = column
    columns[:, HID:] = gain_sum[...]


def finish_first_body(mine, other, up_rest, up_sq, gate, up, rows_sq):
    a = mine[...].astype(F32) + other[...].astype(F32)
    gate[...] = a[:, :HID]
    up[:, : HID - REST] = a[:, HID:]
    up[:, HID - REST :] = up_rest[...]
    s = a * a
    gate_lanes = sum(s[:, k * 128 : (k + 1) * 128] for k in range(5))
    up_lanes = up_sq[...] + sum(s[:, k * 128 : (k + 1) * 128] for k in range(5, FIRST // 128))
    sums = [jnp.sum(lanes.T, axis=0, keepdims=True) for lanes in (gate_lanes, up_lanes)]
    both = jnp.concatenate(sums, axis=0)
    for k in range(8):
        rows_sq[k] = both


def late_sums(sent, arrived):
    late = kernel(late_body, [(sent[3].shape, BF16)] * 2)
    return late(sent[3], arrived[0], sent[4], arrived[1])


def sends_of(sums, arrived, late, columns, halves):
    out = [(128, columns)] * 2 + [(64 if halves else 128, columns), (128, columns)]
    out += [(64, columns)] * halves
    return kernel(turn_body, [(s, BF16) for s in out])(sums, *arrived, *late)


def direct(blocks, move):
    _, one, two, three, *more = blocks
    return [move(one, 1), move(two, 2), move(three, -1)] + [move(m, -2) for m in more]


def joined(own, terms, columns):
    return kernel(join_body, [((128, columns), BF16)])(own, *terms)[0]


def other_replica(a):
    return lax.ppermute(a, "rep", SWAP)


def summed_over(a, move):
    return (a + move(a, -2)) + (move(a, -1) + move(a, 1))


def gathered(parts, move):
    a, b = jnp.concatenate(parts[:2], axis=0), jnp.concatenate(parts[2:], axis=0)
    next_a, next_b, last_a, last_b = move(a, -1), move(b, -1), move(a, 1), move(b, 1)
    return [a, b, next_a, next_b, move(next_a, -1), move(last_b, 1), last_a, last_b]


def on_device(tokens, norm_gain, w_gate, w_up, w_down, cotangent):
    zl, xi, tp = lax.axis_index("zl"), lax.axis_index("x"), lax.axis_index(TP)
    offsets = jnp.arange(16, dtype=jnp.int32)
    order = ((zl + offsets // 4) % 4) * 4 + (xi + offsets % 4) % 4
    gain_f = norm_gain.astype(F32)

    pack_out = [(128, FIRST), (128, SECOND), (64, SECOND), (64, SECOND)]
    pack = kernel(pack_body, [(s, BF16) for s in pack_out])
    first, second, upper, lower = pack(w_gate, w_up, w_down)
    near_first = [first, over_x(first, -1), over_x(first, -2), over_x(first, 1)]
    far = [over_z(upper, -2), over_z(lower, 2)]
    near_second = [second, over_z(second, -1), over_z(second, 1)]
    first = gathered(near_first, over_z)
    near_second.insert(2, jnp.concatenate(far, axis=0))
    second = gathered(near_second, over_x)

    both = copies(jnp.concatenate([tokens, cotangent], axis=0), TP)
    shape, turned = ((ROWS, 2048), BF16), ((2048, ROWS), BF16)
    prepare = kernel(prepare_body, [shape, shape, turned, turned, ((ROWS, 128), F32)], 1, 16)
    normed, dy, normed_t, dy_t, inv = prepare(order, both, gain_f.reshape(8, 1, 256))
    inverse = inv[:, :1]

    out = [((ROWS, 2 * HID), BF16)]
    for columns in (FIRST, SECOND):
        out += [((n, 128, columns), BF16) for n in (4, 4, 4, 2, 2)]
    forward = kernel(
        forward_body,
        out,
        limit=30,
        far=(1, 4, 5, 6, 9, 10),
        scratch=[
            pltpu.VMEM((ROWS, FIRST), F32),
            pltpu.VMEM((ROWS, REST), F32),
            pltpu.VMEM((ROWS, HID), F32),
            pltpu.VMEM((ROWS, HID), BF16),
        ],
    )
    d_pair, *sent = forward(normed, dy, normed_t, dy_t, *first, *second)
    sent_first, sent_second = sent[:5], sent[5:]
    there_first = over_x(sent_first[1], 1), over_x(sent_first[2], -1)
    there_second = over_z(sent_second[1], 1), over_z(sent_second[2], -1)
    late_first = late_sums(sent_first, there_first)
    late_first, there_second = lax.optimization_barrier((late_first, there_second))
    late_second = late_sums(sent_second, there_second)
    late_first = over_x(late_first[0], 1), over_x(late_first[1], -1)
    late_second = over_z(late_second[0], 1), over_z(late_second[1], -1)
    first_blocks = sends_of(sent_first[0], there_first, late_first, FIRST, True)
    second_blocks = sends_of(sent_second[0], there_second, late_second, SECOND, False)
    first_terms = direct(first_blocks, over_z)
    second_terms = direct(second_blocks, over_x)

    input_grad = kernel(input_grad_body, [((8, ROWS, 256), BF16)], 1, 24)
    (shares,) = input_grad(order, d_pair, *first, *second)
    d_normed = jnp.sum(to_each(shares, TP).astype(F32), axis=0)
    local_width = d_normed.shape[1]
    local_gain = lax.dynamic_slice_in_dim(gain_f, tp * local_width, local_width, 0)
    local_tokens = tokens.astype(F32)
    scaled_grad = d_normed * local_gain
    row_part = jnp.sum(scaled_grad * local_tokens, axis=-1)
    gain_part = jnp.sum(d_normed * local_tokens * inverse, axis=0, keepdims=True)
    first_terms, second_terms, row_part, gain_part = lax.optimization_barrier(
        (first_terms, second_terms, row_part, gain_part)
    )
    gain_part = gain_part + other_replica(gain_part)
    first_part = joined(first_blocks[0], first_terms, FIRST)
    second_part = joined(second_blocks[0], second_terms, SECOND)
    first_part, second_part = lax.optimization_barrier((first_part, second_part))
    mine_second = second_part, other_replica(second_part)
    mine_first = first_part, other_replica(first_part)
    rowdot = jnp.sum(copies(row_part, TP), axis=0)
    grad_tokens = (
        cotangent.astype(F32)
        + inverse * scaled_grad
        - local_tokens * inverse**3 * rowdot[:, None] / 2048
    ).astype(BF16)
    square, wide = ((128, 128), F32), ((128, HID), F32)
    finish_second = kernel(
        finish_second_body,
        [((128, REST), F32), square, ((HID, 128), F32), ((1, HID + 256), F32)],
        far=(2,),
    )
    up_rest, up_sq, grad_down, columns = finish_second(*mine_second, gain_part)
    sums = summed_over(summed_over(columns, over_x), over_z)[0]
    down_sq, grad_gain = sums[:HID], sums[HID:]
    finish_first = kernel(finish_first_body, [wide, wide, ((8, 2, 128), F32)], far=(0, 1, 2))
    grad_gate, grad_up, rows_sq = finish_first(*mine_first, up_rest, up_sq)
    gate_up_sq = jnp.sum(to_each(rows_sq, TP), axis=0)
    return (grad_tokens, grad_gain, grad_gate, grad_up, grad_down, gate_up_sq, down_sq)


def solution(mesh):
    fine = Mesh(mesh.devices.reshape(2, 4, 4, 4, 2), ("rep", "zl", "x", "y", "core"))
    rows = ("rep", "zl", "x")
    return jax.shard_map(
        on_device,
        mesh=fine,
        in_specs=(P(rows, TP), P(), P(FS, TP), P(FS, TP), P(TP, FS), P(rows, TP)),
        out_specs=(
            P(rows, TP),
            P(TP),
            P(FS, TP),
            P(FS, TP),
            P(TP, FS),
            P(None, FS),
            P(TP),
        ),
        check_vma=False,
    )
```

```python
import jax
import jax.numpy as jnp
from jax import lax
from jax.experimental import pallas as pl
from jax.experimental.pallas import tpu as pltpu
from jax.sharding import Mesh, PartitionSpec as P


F32 = jnp.float32
BF16 = jnp.bfloat16
TP = ("y", "core")
SWAP = [(0, 1), (1, 0)]
FS = ("zl", "x")
ROWS = 384
HID = 640
FIRST = 896
SECOND = 1024
REST = 2 * HID - FIRST


def over_x(a, shift):
    return lax.ppermute(a, "x", [(i, (i + shift) % 4) for i in range(4)])


def over_z(a, shift):
    return lax.ppermute(a, ("rep", "zl"), [(i, (i + shift) % 8) for i in range(8)])


def over_y(a, shift):
    return lax.ppermute(a, "y", [(i, (i + shift) % 4) for i in range(4)])


def other_core(a):
    return lax.ppermute(a, "core", SWAP)


def to_each(blocks, axis):
    return lax.all_to_all(blocks, axis, 0, 0, tiled=True)


def kernel(body, out, scalars=0, limit=8, scratch=(), far=()):
    whole = pl.BlockSpec(memory_space=pltpu.VMEM)

    def call(*args):
        near = [pltpu.with_memory_space_constraint(a, pltpu.VMEM) for a in args[scalars:]]
        return pl.pallas_call(
            body,
            out_shape=[
                pltpu.HBM(s, d) if i in far else pltpu.VMEM(s, d)
                for i, (s, d) in enumerate(out)
            ],
            in_specs=[pl.BlockSpec(memory_space=pltpu.SMEM)] * scalars + [whole] * len(near),
            out_specs=[whole] * len(out),
            scratch_shapes=list(scratch),
            compiler_params=pltpu.CompilerParams(vmem_limit_bytes=limit << 20),
        )(*args[:scalars], *near)

    return call


def product(left, right):
    return jnp.dot(left, right, preferred_element_type=F32)


def product_last(left, right):
    return lax.dot_general(left, right, (((1,), (1,)), ((), ())), preferred_element_type=F32)


def pack_body(w_gate, w_up, w_down, first, second, upper, lower):
    first[:, :HID] = w_gate[...]
    first[:, HID:] = w_up[:, : FIRST - HID]
    turned = w_down[...].astype(F32).T.astype(BF16)
    for out, at in ((second, slice(0, 128)), (upper, slice(0, 64)), (lower, slice(64, 128))):
        out[:, :REST] = w_up[at, FIRST - HID :]
        out[:, REST:] = turned[at]


def prepare_body(order, places, *refs):
    gain, normed, dy, normed_t, dy_t, inverse, both = refs[8:]
    step = 128
    for k in range(8):
        both[places[k]] = refs[k][...]

    def rows_of(r, carry):
        at = pl.ds(pl.multiple_of(r * step, step), step)
        squares = jnp.zeros((step, 256), F32)
        for t in range(8):
            wide = both[t, at, :].astype(F32)
            squares = squares + wide * wide
        inv = lax.rsqrt(jnp.sum(squares, axis=-1, keepdims=True) / 2048 + 1e-06)
        inverse[at, :] = jnp.broadcast_to(inv, (step, 128))
        below = pl.ds(pl.multiple_of(ROWS + r * step, step), step)
        for j in range(16):
            t = order[j] // 2
            lanes = pl.ds(pl.multiple_of((order[j] % 2) * 128, 128), 128)
            scaled = both[t, at, lanes].astype(F32) * inv * gain[t, :, lanes]
            here = slice(j * 128, (j + 1) * 128)
            normed[at, here] = scaled.astype(BF16)
            normed_t[here, at] = scaled.T.astype(BF16)
            other = both[t, below, lanes]
            dy[at, here] = other
            dy_t[here, at] = other.astype(F32).T.astype(BF16)
        return carry

    lax.fori_loop(0, ROWS // step, rows_of, 0)


def forward_body(*refs):
    normed, dy, normed_t, dy_t = refs[:4]
    first, second = refs[4:12], refs[12:20]
    d_pair = refs[20]
    sent_first, sent_second = refs[21:26], refs[26:31]
    pre, rest, back, hidden = refs[31:]
    for i in range(8):
        term = product(normed[:, i * 256 : (i + 1) * 256], first[i][...])
        pre[...] = term if i == 0 else pre[...] + term
    for i in range(8):
        dx, half = i // 2, i % 2
        a = (8 * half + dx) * 128
        b = a + 512
        pair = jnp.concatenate([normed[:, a : a + 128], normed[:, b : b + 128]], axis=1)
        term = product(pair, second[i][:, :REST])
        rest[...] = term if i == 0 else rest[...] + term
        pair = jnp.concatenate([dy[:, a : a + 128], dy[:, b : b + 128]], axis=1)
        term = product(pair, second[i][:, REST:])
        back[...] = term if i == 0 else back[...] + term

    def gating(r, carry):
        at = pl.ds(pl.multiple_of(r * 32, 32), 32)
        gate = pre[at, :HID]
        up = jnp.concatenate([pre[at, HID:], rest[at, :]], axis=1)
        d_hidden = 0.5 * back[at, :]
        sigma = jax.nn.sigmoid(gate)
        active = gate * sigma
        hidden[at, :] = (active * up).astype(BF16)
        d_pair[at, HID:] = (d_hidden * active).astype(BF16)
        d_pair[at, :HID] = (d_hidden * up * sigma * (1.0 + gate * (1.0 - sigma))).astype(BF16)
        return carry

    lax.fori_loop(0, ROWS // 32, gating, 0)

    def place(sent, group, sub, columns, value):
        own, ahead, behind, late_ahead, late_behind = sent
        low = sub < 2
        if group == 0:
            own[sub, :, columns] = value
        elif group == 1 and low:
            late_ahead[sub, :, columns] = value
        elif group == 1 or (group == 2 and low):
            ahead[sub, :, columns] = value
        elif group == 2:
            behind[sub - 2, :, columns] = value
        elif low:
            behind[sub + 2, :, columns] = value
        else:
            late_behind[sub - 2, :, columns] = value

    for dz in range(4):
        at = slice(dz * 512, (dz + 1) * 512)
        grads = product(normed_t[at, :], d_pair[:, :FIRST]).astype(BF16)
        for dx in range(4):
            place(sent_first, dx, dz, slice(0, FIRST), grads[dx * 128 : (dx + 1) * 128])
        grads = product(normed_t[at, :], d_pair[:, FIRST:]).astype(BF16)
        for dx in range(4):
            place(sent_second, dz, dx, slice(0, REST), grads[dx * 128 : (dx + 1) * 128])
        grads = (0.5 * product(dy_t[at, :], hidden[...])).astype(BF16)
        for dx in range(4):
            place(sent_second, dz, dx, slice(REST, SECOND), grads[dx * 128 : (dx + 1) * 128])


def input_grad_body(order, slots, d_pair, *refs):
    first, second, same, other, out = refs[:8], refs[8:16], *refs[16:]
    for i in range(8):
        dz, half = i // 2, i % 2
        total = product_last(d_pair[:, :FIRST], first[i][...])
        at = slice((dz % 2) * 128, (dz % 2) * 128 + 128)
        pair = [second[(2 * half + k) * 2 + dz // 2][at, :REST] for k in range(2)]
        total = total + product_last(d_pair[:, FIRST:], jnp.concatenate(pair, axis=0))
        for k in range(2):
            j = dz * 4 + half * 2 + k
            lanes = pl.ds(pl.multiple_of((order[j] % 2) * 128, 128), 128)
            out[slots[order[j] // 2], :, lanes] = total[:, k * 128 : (k + 1) * 128].astype(BF16)
    same[...] = out[:4]
    other[...] = out[4:]


def pair_sum_body(same, other, *outs):
    for k in range(4):
        outs[k][...] = (same[k].astype(F32) + other[k].astype(F32)).astype(BF16)


def late_body(kept_ahead, ahead, kept_behind, behind, to_ahead, to_behind):
    half = kept_ahead.shape[0]
    to_ahead[...] = (kept_ahead[...].astype(F32) + ahead[:half].astype(F32)).astype(BF16)
    to_behind[...] = (kept_behind[...].astype(F32) + behind[:half].astype(F32)).astype(BF16)


def turn_body(own, ahead, behind, late_ahead, late_behind, *mine):
    for sub in range(4):
        early, late, at = (behind, late_ahead, sub) if sub < 2 else (ahead, late_behind, sub - 2)
        total = own[sub].astype(F32) + early[at + 2].astype(F32) + late[at].astype(F32)
        total = total.astype(BF16)
        if sub == 2 and len(mine) == 5:
            mine[2][...] = total[:64]
            mine[4][...] = total[64:]
        else:
            mine[sub][...] = total


def join_body(own, ahead, across, behind, *rest):
    far = across[...] if len(rest) == 1 else jnp.concatenate([across[...], rest[0][...]], axis=0)
    pair = own[...].astype(F32) + far.astype(F32)
    rest[-1][...] = (pair + (ahead[...].astype(F32) + behind[...].astype(F32))).astype(BF16)


def finish_second_body(mine, other, gain_sum, up_rest, up_sq, down, columns):
    b = mine[...].astype(F32) + other[...].astype(F32)
    rest, part = b[:, :REST], b[:, REST:]
    up_rest[...] = rest
    s = rest * rest
    up_sq[...] = sum(s[:, k * 128 : (k + 1) * 128] for k in range(REST // 128))
    down[...] = part.T
    column = jnp.sum(part * part, axis=0, keepdims=True)
    columns[:, :HID] = column
    columns[:, HID:] = gain_sum[...]


def finish_first_body(mine, other, up_rest, up_sq, gate, up, rows_sq):
    a = mine[...].astype(F32) + other[...].astype(F32)
    gate[...] = a[:, :HID]
    up[:, : HID - REST] = a[:, HID:]
    up[:, HID - REST :] = up_rest[...]
    s = a * a
    gate_lanes = sum(s[:, k * 128 : (k + 1) * 128] for k in range(5))
    up_lanes = up_sq[...] + sum(s[:, k * 128 : (k + 1) * 128] for k in range(5, FIRST // 128))
    sums = [jnp.sum(lanes.T, axis=0, keepdims=True) for lanes in (gate_lanes, up_lanes)]
    both = jnp.concatenate(sums, axis=0)
    for k in range(8):
        rows_sq[k] = both


def late_sums(sent, arrived):
    late = kernel(late_body, [(sent[3].shape, BF16)] * 2)
    return late(sent[3], arrived[0], sent[4], arrived[1])


def sends_of(sums, arrived, late, columns, halves):
    out = [(128, columns)] * 2 + [(64 if halves else 128, columns), (128, columns)]
    out += [(64, columns)] * halves
    return kernel(turn_body, [(s, BF16) for s in out])(sums, *arrived, *late)


def direct(blocks, move):
    _, one, two, three, *more = blocks
    return [move(one, 1), move(two, 2), move(three, -1)] + [move(m, -2) for m in more]


def joined(own, terms, columns):
    return kernel(join_body, [((128, columns), BF16)])(own, *terms)[0]


def other_replica(a):
    return lax.ppermute(a, "rep", SWAP)


def summed_over(a, move):
    return (a + move(a, -2)) + (move(a, -1) + move(a, 1))


def group_body(own, *refs):
    a, b = refs[-2:]
    a[:128] = own[...]
    a[128:] = refs[0][...]
    far = refs[1:-3]
    step = 128 // len(far)
    for k, part in enumerate(far):
        b[k * step : (k + 1) * step] = part[...]
    b[128:] = refs[-3][...]


def gathered(parts, move):
    columns = parts[0].shape[1]
    a, b = kernel(group_body, [((256, columns), BF16)] * 2)(*parts)
    next_a, next_b, last_a, last_b = move(a, -1), move(b, -1), move(a, 1), move(b, 1)
    far_a, far_b = move(next_a, -1), move(last_b, 1)
    return [a, b, next_a, next_b, far_a, far_b, last_a, last_b]


def on_device(tokens, norm_gain, w_gate, w_up, w_down, cotangent):
    zl, xi, tp = lax.axis_index("zl"), lax.axis_index("x"), lax.axis_index(TP)
    offsets = jnp.arange(16, dtype=jnp.int32)
    order = ((zl + offsets // 4) % 4) * 4 + (xi + offsets % 4) % 4
    gain_f = norm_gain.astype(F32)
    yi, ci = lax.axis_index("y"), lax.axis_index("core")
    eight = jnp.arange(8, dtype=jnp.int32)
    places = (yi + eight % 4) % 4 * 2 + (ci + eight // 4) % 2
    slots = (eight // 2 + 4 - yi) % 4 + (eight + ci) % 2 * 4

    pack_out = [(128, FIRST), (128, SECOND), (64, SECOND), (64, SECOND)]
    pack = kernel(pack_body, [(s, BF16) for s in pack_out])
    first, second, upper, lower = pack(w_gate, w_up, w_down)
    near_first = [first, over_x(first, -1), over_x(first, -2), over_x(first, 1)]
    far = [over_z(upper, -2), over_z(lower, 2)]
    near_second = [second, over_z(second, -1), *far, over_z(second, 1)]
    first = gathered(near_first, over_z)
    second = gathered(near_second, over_x)

    mine = jnp.concatenate([tokens, cotangent], axis=0)
    both = [mine, over_y(mine, -1), over_y(mine, -2), over_y(mine, 1)]
    both += [other_core(b) for b in both]
    shape, turned = ((ROWS, 2048), BF16), ((2048, ROWS), BF16)
    prepare = kernel(
        prepare_body,
        [shape, shape, turned, turned, ((ROWS, 128), F32)],
        2,
        16,
        scratch=[pltpu.VMEM((8, 2 * ROWS, 256), BF16)],
    )
    normed, dy, normed_t, dy_t, inv = prepare(order, places, *both, gain_f.reshape(8, 1, 256))
    inverse = inv[:, :1]

    out = [((ROWS, 2 * HID), BF16)]
    for columns in (FIRST, SECOND):
        out += [((n, 128, columns), BF16) for n in (4, 4, 4, 2, 2)]
    forward = kernel(
        forward_body,
        out,
        limit=20,
        scratch=[
            pltpu.VMEM((ROWS, FIRST), F32),
            pltpu.VMEM((ROWS, REST), F32),
            pltpu.VMEM((ROWS, HID), F32),
            pltpu.VMEM((ROWS, HID), BF16),
        ],
    )
    d_pair, *sent = forward(normed, dy, normed_t, dy_t, *first, *second)
    sent_first, sent_second = sent[:5], sent[5:]
    there_first = over_x(sent_first[1], 1), over_x(sent_first[2], -1)
    there_second = over_z(sent_second[1], 1), over_z(sent_second[2], -1)
    late_first = late_sums(sent_first, there_first)
    late_first, there_second = lax.optimization_barrier((late_first, there_second))
    late_second = late_sums(sent_second, there_second)
    late_first = over_x(late_first[0], 1), over_x(late_first[1], -1)
    late_second = over_z(late_second[0], 1), over_z(late_second[1], -1)
    first_blocks = sends_of(sent_first[0], there_first, late_first, FIRST, True)
    second_blocks = sends_of(sent_second[0], there_second, late_second, SECOND, False)
    first_terms = direct(first_blocks, over_z)
    second_terms = direct(second_blocks, over_x)

    share = ((4, ROWS, 256), BF16)
    input_grad = kernel(
        input_grad_body, [share, share], 2, 16, scratch=[pltpu.VMEM((8, ROWS, 256), BF16)]
    )
    same, other = input_grad(order, slots, d_pair, *first, *second)
    pair_sum = kernel(pair_sum_body, [((ROWS, 256), BF16)] * 4)
    near, one, two, three = pair_sum(same, other_core(other))
    shares = near, over_y(one, 1), over_y(two, 2), over_y(three, -1)
    d_normed = sum(s.astype(F32) for s in shares)
    local_width = d_normed.shape[1]
    local_gain = lax.dynamic_slice_in_dim(gain_f, tp * local_width, local_width, 0)
    local_tokens = tokens.astype(F32)
    scaled_grad = d_normed * local_gain
    row_part = jnp.sum(scaled_grad * local_tokens, axis=-1)
    gain_part = jnp.sum(d_normed * local_tokens * inverse, axis=0, keepdims=True)
    first_terms, second_terms, row_part, gain_part = lax.optimization_barrier(
        (first_terms, second_terms, row_part, gain_part)
    )
    gain_part = gain_part + other_replica(gain_part)
    first_part = joined(first_blocks[0], first_terms, FIRST)
    second_part = joined(second_blocks[0], second_terms, SECOND)
    first_part, second_part = lax.optimization_barrier((first_part, second_part))
    mine_second = second_part, other_replica(second_part)
    mine_first = first_part, other_replica(first_part)
    row_part = row_part.reshape(3, 128)
    rowdot = summed_over(row_part + other_core(row_part), over_y).reshape(ROWS)
    grad_tokens = (
        cotangent.astype(F32)
        + inverse * scaled_grad
        - local_tokens * inverse**3 * rowdot[:, None] / 2048
    ).astype(BF16)
    square, wide = ((128, 128), F32), ((128, HID), F32)
    finish_second = kernel(
        finish_second_body,
        [((128, REST), F32), square, ((HID, 128), F32), ((1, HID + 256), F32)],
        far=(2,),
    )
    up_rest, up_sq, grad_down, columns = finish_second(*mine_second, gain_part)
    sums = summed_over(summed_over(columns, over_x), over_z)[0]
    down_sq, grad_gain = sums[:HID], sums[HID:]
    finish_first = kernel(finish_first_body, [wide, wide, ((8, 2, 128), F32)], far=(0, 1, 2))
    grad_gate, grad_up, rows_sq = finish_first(*mine_first, up_rest, up_sq)
    gate_up_sq = jnp.sum(to_each(rows_sq, TP), axis=0)
    return (grad_tokens, grad_gain, grad_gate, grad_up, grad_down, gate_up_sq, down_sq)


def solution(mesh):
    fine = Mesh(mesh.devices.reshape(2, 4, 4, 4, 2), ("rep", "zl", "x", "y", "core"))
    rows = ("rep", "zl", "x")
    return jax.shard_map(
        on_device,
        mesh=fine,
        in_specs=(P(rows, TP), P(), P(FS, TP), P(FS, TP), P(TP, FS), P(rows, TP)),
        out_specs=(
            P(rows, TP),
            P(TP),
            P(FS, TP),
            P(FS, TP),
            P(TP, FS),
            P(None, FS),
            P(TP),
        ),
        check_vma=False,
    )
```

```python
import jax
import jax.numpy as jnp
from jax import lax
from jax.experimental import pallas as pl
from jax.experimental.pallas import tpu as pltpu
from jax.sharding import Mesh, PartitionSpec as P


F32 = jnp.float32
BF16 = jnp.bfloat16
TP = ("y", "core")
SWAP = [(0, 1), (1, 0)]
FS = ("zl", "x")
ROWS = 384
HID = 640
FIRST = 896
SECOND = 1024
REST = 2 * HID - FIRST


def over_x(a, shift):
    return lax.ppermute(a, "x", [(i, (i + shift) % 4) for i in range(4)])


def over_z(a, shift):
    return lax.ppermute(a, ("rep", "zl"), [(i, (i + shift) % 8) for i in range(8)])


def over_y(a, shift):
    return lax.ppermute(a, "y", [(i, (i + shift) % 4) for i in range(4)])


def other_core(a):
    return lax.ppermute(a, "core", SWAP)


def to_each(blocks, axis):
    return lax.all_to_all(blocks, axis, 0, 0, tiled=True)


def kernel(body, out, scalars=0, limit=8, scratch=(), far=()):
    whole = pl.BlockSpec(memory_space=pltpu.VMEM)

    def call(*args):
        near = [pltpu.with_memory_space_constraint(a, pltpu.VMEM) for a in args[scalars:]]
        return pl.pallas_call(
            body,
            out_shape=[
                pltpu.HBM(s, d) if i in far else pltpu.VMEM(s, d)
                for i, (s, d) in enumerate(out)
            ],
            in_specs=[pl.BlockSpec(memory_space=pltpu.SMEM)] * scalars + [whole] * len(near),
            out_specs=[whole] * len(out),
            scratch_shapes=list(scratch),
            compiler_params=pltpu.CompilerParams(vmem_limit_bytes=limit << 20),
        )(*args[:scalars], *near)

    return call


def product(left, right):
    return jnp.dot(left, right, preferred_element_type=F32)


def product_last(left, right):
    return lax.dot_general(left, right, (((1,), (1,)), ((), ())), preferred_element_type=F32)


def pack_body(w_gate, w_up, w_down, first, second, upper, lower):
    first[:, :HID] = w_gate[...]
    first[:, HID:] = w_up[:, : FIRST - HID]
    turned = w_down[...].astype(F32).T.astype(BF16)
    for out, at in ((second, slice(0, 128)), (upper, slice(0, 64)), (lower, slice(64, 128))):
        out[:, :REST] = w_up[at, FIRST - HID :]
        out[:, REST:] = turned[at]


def prepare_body(order, places, *refs):
    gain, normed, dy, normed_t, dy_t, inverse, both = refs[8:]
    step = 128
    for k in range(8):
        both[places[k]] = refs[k][...]

    def rows_of(r, carry):
        at = pl.ds(pl.multiple_of(r * step, step), step)
        squares = jnp.zeros((step, 256), F32)
        for t in range(8):
            wide = both[t, at, :].astype(F32)
            squares = squares + wide * wide
        inv = lax.rsqrt(jnp.sum(squares, axis=-1, keepdims=True) / 2048 + 1e-06)
        inverse[at, :] = jnp.broadcast_to(inv, (step, 128))
        below = pl.ds(pl.multiple_of(ROWS + r * step, step), step)
        for j in range(16):
            t = order[j] // 2
            lanes = pl.ds(pl.multiple_of((order[j] % 2) * 128, 128), 128)
            scaled = both[t, at, lanes].astype(F32) * inv * gain[t, :, lanes]
            here = slice(j * 128, (j + 1) * 128)
            normed[at, here] = scaled.astype(BF16)
            normed_t[here, at] = scaled.T.astype(BF16)
            other = both[t, below, lanes]
            dy[at, here] = other
            dy_t[here, at] = other.astype(F32).T.astype(BF16)
        return carry

    lax.fori_loop(0, ROWS // step, rows_of, 0)


def forward_body(*refs):
    normed, dy, normed_t, dy_t = refs[:4]
    first, second = refs[4:12], refs[12:20]
    d_pair = refs[20]
    sent_first, sent_second = refs[21:26], refs[26:31]
    pre, rest, back, hidden = refs[31:]
    for i in range(8):
        term = product(normed[:, i * 256 : (i + 1) * 256], first[i][...])
        pre[...] = term if i == 0 else pre[...] + term
    for i in range(8):
        dx, half = i // 2, i % 2
        a = (8 * half + dx) * 128
        b = a + 512
        pair = jnp.concatenate([normed[:, a : a + 128], normed[:, b : b + 128]], axis=1)
        term = product(pair, second[i][:, :REST])
        rest[...] = term if i == 0 else rest[...] + term
        pair = jnp.concatenate([dy[:, a : a + 128], dy[:, b : b + 128]], axis=1)
        term = product(pair, second[i][:, REST:])
        back[...] = term if i == 0 else back[...] + term

    def gating(r, carry):
        at = pl.ds(pl.multiple_of(r * 32, 32), 32)
        gate = pre[at, :HID]
        up = jnp.concatenate([pre[at, HID:], rest[at, :]], axis=1)
        d_hidden = 0.5 * back[at, :]
        sigma = jax.nn.sigmoid(gate)
        active = gate * sigma
        hidden[at, :] = (active * up).astype(BF16)
        d_pair[at, HID:] = (d_hidden * active).astype(BF16)
        d_pair[at, :HID] = (d_hidden * up * sigma * (1.0 + gate * (1.0 - sigma))).astype(BF16)
        return carry

    lax.fori_loop(0, ROWS // 32, gating, 0)

    def place(sent, group, sub, columns, value):
        own, ahead, behind, late_ahead, late_behind = sent
        low = sub < 2
        if group == 0:
            own[sub, :, columns] = value
        elif group == 1 and low:
            late_ahead[sub, :, columns] = value
        elif group == 1 or (group == 2 and low):
            ahead[sub, :, columns] = value
        elif group == 2:
            behind[sub - 2, :, columns] = value
        elif low:
            behind[sub + 2, :, columns] = value
        else:
            late_behind[sub - 2, :, columns] = value

    for dz in range(4):
        at = slice(dz * 512, (dz + 1) * 512)
        grads = product(normed_t[at, :], d_pair[:, :FIRST]).astype(BF16)
        for dx in range(4):
            place(sent_first, dx, dz, slice(0, FIRST), grads[dx * 128 : (dx + 1) * 128])
        grads = product(normed_t[at, :], d_pair[:, FIRST:]).astype(BF16)
        for dx in range(4):
            place(sent_second, dz, dx, slice(0, REST), grads[dx * 128 : (dx + 1) * 128])
        grads = (0.5 * product(dy_t[at, :], hidden[...])).astype(BF16)
        for dx in range(4):
            place(sent_second, dz, dx, slice(REST, SECOND), grads[dx * 128 : (dx + 1) * 128])


def input_grad_body(order, slots, d_pair, *refs):
    first, second, same, other, out = refs[:8], refs[8:16], *refs[16:]
    for i in range(8):
        dz, half = i // 2, i % 2
        total = product_last(d_pair[:, :FIRST], first[i][...])
        at = slice((dz % 2) * 128, (dz % 2) * 128 + 128)
        pair = [second[(2 * half + k) * 2 + dz // 2][at, :REST] for k in range(2)]
        total = total + product_last(d_pair[:, FIRST:], jnp.concatenate(pair, axis=0))
        for k in range(2):
            j = dz * 4 + half * 2 + k
            lanes = pl.ds(pl.multiple_of((order[j] % 2) * 128, 128), 128)
            out[slots[order[j] // 2], :, lanes] = total[:, k * 128 : (k + 1) * 128].astype(BF16)
    same[...] = out[:4]
    other[...] = out[4:]


def pair_sum_body(same, other, *outs):
    for k in range(4):
        outs[k][...] = (same[k].astype(F32) + other[k].astype(F32)).astype(BF16)


def late_body(kept_ahead, ahead, kept_behind, behind, to_ahead, to_behind):
    half = kept_ahead.shape[0]
    to_ahead[...] = (kept_ahead[...].astype(F32) + ahead[:half].astype(F32)).astype(BF16)
    to_behind[...] = (kept_behind[...].astype(F32) + behind[:half].astype(F32)).astype(BF16)


def turn_body(own, ahead, behind, late_ahead, late_behind, *mine):
    for sub in range(4):
        early, late, at = (behind, late_ahead, sub) if sub < 2 else (ahead, late_behind, sub - 2)
        total = own[sub].astype(F32) + early[at + 2].astype(F32) + late[at].astype(F32)
        total = total.astype(BF16)
        if sub == 2 and len(mine) == 5:
            mine[2][...] = total[:64]
            mine[4][...] = total[64:]
        else:
            mine[sub][...] = total


def join_body(own, ahead, across, behind, *rest):
    far = across[...] if len(rest) == 1 else jnp.concatenate([across[...], rest[0][...]], axis=0)
    pair = own[...].astype(F32) + far.astype(F32)
    rest[-1][...] = (pair + (ahead[...].astype(F32) + behind[...].astype(F32))).astype(BF16)


def finish_second_body(mine, other, gain_sum, up_rest, up_sq, down, columns):
    b = mine[...].astype(F32) + other[...].astype(F32)
    rest, part = b[:, :REST], b[:, REST:]
    up_rest[...] = rest
    s = rest * rest
    up_sq[...] = sum(s[:, k * 128 : (k + 1) * 128] for k in range(REST // 128))
    down[...] = part.T
    column = jnp.sum(part * part, axis=0, keepdims=True)
    for k in range(16):
        columns[k, :, :HID] = column
        columns[k, :, HID:] = gain_sum[...]


def finish_first_body(mine, other, up_rest, up_sq, gate, up, rows_sq):
    a = mine[...].astype(F32) + other[...].astype(F32)
    gate[...] = a[:, :HID]
    up[:, : HID - REST] = a[:, HID:]
    up[:, HID - REST :] = up_rest[...]
    s = a * a
    gate_lanes = sum(s[:, k * 128 : (k + 1) * 128] for k in range(5))
    up_lanes = up_sq[...] + sum(s[:, k * 128 : (k + 1) * 128] for k in range(5, FIRST // 128))
    sums = [jnp.sum(lanes.T, axis=0, keepdims=True) for lanes in (gate_lanes, up_lanes)]
    both = jnp.concatenate(sums, axis=0)
    rows_sq[...] = both


def late_sums(sent, arrived):
    late = kernel(late_body, [(sent[3].shape, BF16)] * 2)
    return late(sent[3], arrived[0], sent[4], arrived[1])


def sends_of(sums, arrived, late, columns, halves):
    out = [(128, columns)] * 2 + [(64 if halves else 128, columns), (128, columns)]
    out += [(64, columns)] * halves
    return kernel(turn_body, [(s, BF16) for s in out])(sums, *arrived, *late)


def direct(blocks, move):
    _, one, two, three, *more = blocks
    return [move(one, 1), move(two, 2), move(three, -1)] + [move(m, -2) for m in more]


def joined(own, terms, columns):
    return kernel(join_body, [((128, columns), BF16)])(own, *terms)[0]


def other_replica(a):
    return lax.ppermute(a, "rep", SWAP)


def summed_over(a, move):
    return (a + move(a, -2)) + (move(a, -1) + move(a, 1))


def group_body(own, *refs):
    a, b = refs[-2:]
    a[:128] = own[...]
    a[128:] = refs[0][...]
    far = refs[1:-3]
    step = 128 // len(far)
    for k, part in enumerate(far):
        b[k * step : (k + 1) * step] = part[...]
    b[128:] = refs[-3][...]


def gathered(parts, move):
    columns = parts[0].shape[1]
    a, b = kernel(group_body, [((256, columns), BF16)] * 2)(*parts)
    next_a, next_b, last_a, last_b = move(a, -1), move(b, -1), move(a, 1), move(b, 1)
    far_a, far_b = move(next_a, -1), move(last_b, 1)
    return [a, b, next_a, next_b, far_a, far_b, last_a, last_b]


def on_device(tokens, norm_gain, w_gate, w_up, w_down, cotangent):
    zl, xi, tp = lax.axis_index("zl"), lax.axis_index("x"), lax.axis_index(TP)
    offsets = jnp.arange(16, dtype=jnp.int32)
    order = ((zl + offsets // 4) % 4) * 4 + (xi + offsets % 4) % 4
    gain_f = norm_gain.astype(F32)
    yi, ci = lax.axis_index("y"), lax.axis_index("core")
    eight = jnp.arange(8, dtype=jnp.int32)
    places = (yi + eight % 4) % 4 * 2 + (ci + eight // 4) % 2
    slots = (eight // 2 + 4 - yi) % 4 + (eight + ci) % 2 * 4

    pack_out = [(128, FIRST), (128, SECOND), (64, SECOND), (64, SECOND)]
    pack = kernel(pack_body, [(s, BF16) for s in pack_out])
    first, second, upper, lower = pack(w_gate, w_up, w_down)
    near_first = [first, over_x(first, -1), over_x(first, -2), over_x(first, 1)]
    far = [over_z(upper, -2), over_z(lower, 2)]
    near_second = [second, over_z(second, -1), *far, over_z(second, 1)]
    first = gathered(near_first, over_z)
    second = gathered(near_second, over_x)

    mine = jnp.concatenate([tokens, cotangent], axis=0)
    both = [mine, over_y(mine, -1), over_y(mine, -2), over_y(mine, 1)]
    both += [other_core(b) for b in both]
    shape, turned = ((ROWS, 2048), BF16), ((2048, ROWS), BF16)
    prepare = kernel(
        prepare_body,
        [shape, shape, turned, turned, ((ROWS, 128), F32)],
        2,
        16,
        scratch=[pltpu.VMEM((8, 2 * ROWS, 256), BF16)],
    )
    normed, dy, normed_t, dy_t, inv = prepare(order, places, *both, gain_f.reshape(8, 1, 256))
    inverse = inv[:, :1]

    out = [((ROWS, 2 * HID), BF16)]
    for columns in (FIRST, SECOND):
        out += [((n, 128, columns), BF16) for n in (4, 4, 4, 2, 2)]
    forward = kernel(
        forward_body,
        out,
        limit=20,
        scratch=[
            pltpu.VMEM((ROWS, FIRST), F32),
            pltpu.VMEM((ROWS, REST), F32),
            pltpu.VMEM((ROWS, HID), F32),
            pltpu.VMEM((ROWS, HID), BF16),
        ],
    )
    d_pair, *sent = forward(normed, dy, normed_t, dy_t, *first, *second)
    sent_first, sent_second = sent[:5], sent[5:]
    there_first = over_x(sent_first[1], 1), over_x(sent_first[2], -1)
    there_second = over_z(sent_second[1], 1), over_z(sent_second[2], -1)
    late_first = late_sums(sent_first, there_first)
    late_second = late_sums(sent_second, there_second)
    late_first = over_x(late_first[0], 1), over_x(late_first[1], -1)
    late_second = over_z(late_second[0], 1), over_z(late_second[1], -1)
    first_blocks = sends_of(sent_first[0], there_first, late_first, FIRST, True)
    second_blocks = sends_of(sent_second[0], there_second, late_second, SECOND, False)
    first_terms = direct(first_blocks, over_z)
    second_terms = direct(second_blocks, over_x)

    share = ((4, ROWS, 256), BF16)
    input_grad = kernel(
        input_grad_body, [share, share], 2, 16, scratch=[pltpu.VMEM((8, ROWS, 256), BF16)]
    )
    same, other = input_grad(order, slots, d_pair, *first, *second)
    pair_sum = kernel(pair_sum_body, [((ROWS, 256), BF16)] * 4)
    near, one, two, three = pair_sum(same, other_core(other))
    shares = near, over_y(one, 1), over_y(two, 2), over_y(three, -1)
    d_normed = sum(s.astype(F32) for s in shares)
    local_width = d_normed.shape[1]
    local_gain = lax.dynamic_slice_in_dim(gain_f, tp * local_width, local_width, 0)
    local_tokens = tokens.astype(F32)
    scaled_grad = d_normed * local_gain
    row_part = jnp.sum(scaled_grad * local_tokens, axis=-1)
    gain_part = jnp.sum(d_normed * local_tokens * inverse, axis=0, keepdims=True)
    gain_part = gain_part + other_replica(gain_part)
    first_part = joined(first_blocks[0], first_terms, FIRST)
    second_part = joined(second_blocks[0], second_terms, SECOND)
    mine_second = second_part, other_replica(second_part)
    mine_first = first_part, other_replica(first_part)
    row_part = row_part.reshape(3, 128)
    rowdot = summed_over(row_part + other_core(row_part), over_y).reshape(ROWS)
    grad_tokens = (
        cotangent.astype(F32)
        + inverse * scaled_grad
        - local_tokens * inverse**3 * rowdot[:, None] / 2048
    ).astype(BF16)
    square, wide = ((128, 128), F32), ((128, HID), F32)
    finish_second = kernel(
        finish_second_body,
        [((128, REST), F32), square, ((HID, 128), F32), ((16, 1, HID + 256), F32)],
        far=(2, 3),
    )
    up_rest, up_sq, grad_down, columns = finish_second(*mine_second, gain_part)
    sums = jnp.sum(to_each(columns, FS), axis=0)[0]
    down_sq, grad_gain = sums[:HID], sums[HID:]
    finish_first = kernel(finish_first_body, [wide, wide, ((2, 128), F32)], far=(0, 1))
    grad_gate, grad_up, rows_sq = finish_first(*mine_first, up_rest, up_sq)
    gate_up_sq = summed_over(rows_sq + other_core(rows_sq), over_y)
    return (grad_tokens, grad_gain, grad_gate, grad_up, grad_down, gate_up_sq, down_sq)


def solution(mesh):
    fine = Mesh(mesh.devices.reshape(2, 4, 4, 4, 2), ("rep", "zl", "x", "y", "core"))
    rows = ("rep", "zl", "x")
    return jax.shard_map(
        on_device,
        mesh=fine,
        in_specs=(P(rows, TP), P(), P(FS, TP), P(FS, TP), P(TP, FS), P(rows, TP)),
        out_specs=(
            P(rows, TP),
            P(TP),
            P(FS, TP),
            P(FS, TP),
            P(TP, FS),
            P(None, FS),
            P(TP),
        ),
        check_vma=False,
    )
```

```python
import jax
import jax.numpy as jnp
from jax import lax
from jax.experimental import pallas as pl
from jax.experimental.pallas import tpu as pltpu
from jax.sharding import Mesh, PartitionSpec as P


F32 = jnp.float32
BF16 = jnp.bfloat16
TP = ("y", "core")
SWAP = [(0, 1), (1, 0)]
FS = ("zl", "x")
ROWS = 384
HID = 640
FIRST = 896
SECOND = 1024
REST = 2 * HID - FIRST


def over_x(a, shift):
    return lax.ppermute(a, "x", [(i, (i + shift) % 4) for i in range(4)])


def over_z(a, shift):
    return lax.ppermute(a, ("rep", "zl"), [(i, (i + shift) % 8) for i in range(8)])


def over_y(a, shift):
    return lax.ppermute(a, "y", [(i, (i + shift) % 4) for i in range(4)])


def other_core(a):
    return lax.ppermute(a, "core", SWAP)


def to_each(blocks, axis):
    return lax.all_to_all(blocks, axis, 0, 0, tiled=True)


def kernel(body, out, scalars=0, limit=8, scratch=(), far=()):
    whole = pl.BlockSpec(memory_space=pltpu.VMEM)

    def call(*args):
        near = [pltpu.with_memory_space_constraint(a, pltpu.VMEM) for a in args[scalars:]]
        return pl.pallas_call(
            body,
            out_shape=[
                pltpu.HBM(s, d) if i in far else pltpu.VMEM(s, d)
                for i, (s, d) in enumerate(out)
            ],
            in_specs=[pl.BlockSpec(memory_space=pltpu.SMEM)] * scalars + [whole] * len(near),
            out_specs=[whole] * len(out),
            scratch_shapes=list(scratch),
            compiler_params=pltpu.CompilerParams(vmem_limit_bytes=limit << 20),
        )(*args[:scalars], *near)

    return call


def product(left, right):
    return jnp.dot(left, right, preferred_element_type=F32)


def product_last(left, right):
    return lax.dot_general(left, right, (((1,), (1,)), ((), ())), preferred_element_type=F32)


def pack_body(w_gate, w_up, w_down, first, second, upper, lower):
    first[:, :HID] = w_gate[...]
    first[:, HID:] = w_up[:, : FIRST - HID]
    turned = w_down[...].astype(F32).T.astype(BF16)
    for out, at in ((second, slice(0, 128)), (upper, slice(0, 64)), (lower, slice(64, 128))):
        out[:, :REST] = w_up[at, FIRST - HID :]
        out[:, REST:] = turned[at]


def prepare_body(order, places, *refs):
    gain, normed, dy, normed_t, dy_t, inverse, both = refs[8:]
    step = 128
    for k in range(8):
        both[places[k]] = refs[k][...]

    def rows_of(r, carry):
        at = pl.ds(pl.multiple_of(r * step, step), step)
        squares = jnp.zeros((step, 256), F32)
        for t in range(8):
            wide = both[t, at, :].astype(F32)
            squares = squares + wide * wide
        inv = lax.rsqrt(jnp.sum(squares, axis=-1, keepdims=True) / 2048 + 1e-06)
        inverse[at, :] = jnp.broadcast_to(inv, (step, 128))
        below = pl.ds(pl.multiple_of(ROWS + r * step, step), step)
        for j in range(16):
            t = order[j] // 2
            lanes = pl.ds(pl.multiple_of((order[j] % 2) * 128, 128), 128)
            scaled = both[t, at, lanes].astype(F32) * inv * gain[t, :, lanes]
            here = slice(j * 128, (j + 1) * 128)
            normed[at, here] = scaled.astype(BF16)
            normed_t[here, at] = scaled.T.astype(BF16)
            other = both[t, below, lanes]
            dy[at, here] = other
            dy_t[here, at] = other.astype(F32).T.astype(BF16)
        return carry

    lax.fori_loop(0, ROWS // step, rows_of, 0)


def forward_body(*refs):
    normed, dy, normed_t, dy_t = refs[:4]
    first, second = refs[4:12], refs[12:20]
    d_pair = refs[20]
    sent_first, sent_second = refs[21:26], refs[26:31]
    pre, rest, back, hidden = refs[31:]
    for i in range(8):
        term = product(normed[:, i * 256 : (i + 1) * 256], first[i][...])
        pre[...] = term if i == 0 else pre[...] + term
    for i in range(8):
        dx, half = i // 2, i % 2
        a = (8 * half + dx) * 128
        b = a + 512
        pair = jnp.concatenate([normed[:, a : a + 128], normed[:, b : b + 128]], axis=1)
        term = product(pair, second[i][:, :REST])
        rest[...] = term if i == 0 else rest[...] + term
        pair = jnp.concatenate([dy[:, a : a + 128], dy[:, b : b + 128]], axis=1)
        term = product(pair, second[i][:, REST:])
        back[...] = term if i == 0 else back[...] + term

    def gating(r, carry):
        at = pl.ds(pl.multiple_of(r * 32, 32), 32)
        gate = pre[at, :HID]
        up = jnp.concatenate([pre[at, HID:], rest[at, :]], axis=1)
        d_hidden = 0.5 * back[at, :]
        sigma = jax.nn.sigmoid(gate)
        active = gate * sigma
        hidden[at, :] = (active * up).astype(BF16)
        d_pair[at, HID:] = (d_hidden * active).astype(BF16)
        d_pair[at, :HID] = (d_hidden * up * sigma * (1.0 + gate * (1.0 - sigma))).astype(BF16)
        return carry

    lax.fori_loop(0, ROWS // 32, gating, 0)

    def place(sent, group, sub, columns, value):
        own, ahead, behind, late_ahead, late_behind = sent
        low = sub < 2
        if group == 0:
            own[sub, :, columns] = value
        elif group == 1 and low:
            late_ahead[sub, :, columns] = value
        elif group == 1 or (group == 2 and low):
            ahead[sub, :, columns] = value
        elif group == 2:
            behind[sub - 2, :, columns] = value
        elif low:
            behind[sub + 2, :, columns] = value
        else:
            late_behind[sub - 2, :, columns] = value

    for dz in range(4):
        at = slice(dz * 512, (dz + 1) * 512)
        grads = product(normed_t[at, :], d_pair[:, :FIRST]).astype(BF16)
        for dx in range(4):
            place(sent_first, dx, dz, slice(0, FIRST), grads[dx * 128 : (dx + 1) * 128])
        grads = product(normed_t[at, :], d_pair[:, FIRST:]).astype(BF16)
        for dx in range(4):
            place(sent_second, dz, dx, slice(0, REST), grads[dx * 128 : (dx + 1) * 128])
        grads = (0.5 * product(dy_t[at, :], hidden[...])).astype(BF16)
        for dx in range(4):
            place(sent_second, dz, dx, slice(REST, SECOND), grads[dx * 128 : (dx + 1) * 128])


def input_grad_body(order, slots, d_pair, *refs):
    first, second, same, other, out = refs[:8], refs[8:16], *refs[16:]
    for i in range(8):
        dz, half = i // 2, i % 2
        total = product_last(d_pair[:, :FIRST], first[i][...])
        at = slice((dz % 2) * 128, (dz % 2) * 128 + 128)
        pair = [second[(2 * half + k) * 2 + dz // 2][at, :REST] for k in range(2)]
        total = total + product_last(d_pair[:, FIRST:], jnp.concatenate(pair, axis=0))
        for k in range(2):
            j = dz * 4 + half * 2 + k
            lanes = pl.ds(pl.multiple_of((order[j] % 2) * 128, 128), 128)
            out[slots[order[j] // 2], :, lanes] = total[:, k * 128 : (k + 1) * 128].astype(BF16)
    same[...] = out[:4]
    other[...] = out[4:]


def pair_sum_body(same, other, *outs):
    for k in range(4):
        outs[k][...] = (same[k].astype(F32) + other[k].astype(F32)).astype(BF16)


def late_body(kept_ahead, ahead, kept_behind, behind, to_ahead, to_behind):
    half = kept_ahead.shape[0]
    to_ahead[...] = (kept_ahead[...].astype(F32) + ahead[:half].astype(F32)).astype(BF16)
    to_behind[...] = (kept_behind[...].astype(F32) + behind[:half].astype(F32)).astype(BF16)


def turn_body(own, ahead, behind, late_ahead, late_behind, *mine):
    for sub in range(4):
        early, late, at = (behind, late_ahead, sub) if sub < 2 else (ahead, late_behind, sub - 2)
        total = own[sub].astype(F32) + early[at + 2].astype(F32) + late[at].astype(F32)
        total = total.astype(BF16)
        if sub == 2 and len(mine) == 5:
            mine[2][...] = total[:64]
            mine[4][...] = total[64:]
        else:
            mine[sub][...] = total


def join_body(own, ahead, across, behind, *rest):
    far = across[...] if len(rest) == 1 else jnp.concatenate([across[...], rest[0][...]], axis=0)
    pair = own[...].astype(F32) + far.astype(F32)
    rest[-1][...] = (pair + (ahead[...].astype(F32) + behind[...].astype(F32))).astype(BF16)


def finish_second_body(mine, other, gain_sum, up_rest, up_sq, down, columns):
    b = mine[...].astype(F32) + other[...].astype(F32)
    rest, part = b[:, :REST], b[:, REST:]
    up_rest[...] = rest
    s = rest * rest
    up_sq[...] = sum(s[:, k * 128 : (k + 1) * 128] for k in range(REST // 128))
    down[...] = part.T
    column = jnp.sum(part * part, axis=0, keepdims=True)
    for k in range(16):
        columns[k, :, :HID] = column
        columns[k, :, HID:] = gain_sum[...]


def finish_first_body(mine, other, up_rest, up_sq, gate, up, rows_sq):
    a = mine[...].astype(F32) + other[...].astype(F32)
    gate[...] = a[:, :HID]
    up[:, : HID - REST] = a[:, HID:]
    up[:, HID - REST :] = up_rest[...]
    s = a * a
    gate_lanes = sum(s[:, k * 128 : (k + 1) * 128] for k in range(5))
    up_lanes = up_sq[...] + sum(s[:, k * 128 : (k + 1) * 128] for k in range(5, FIRST // 128))
    sums = [jnp.sum(lanes.T, axis=0, keepdims=True) for lanes in (gate_lanes, up_lanes)]
    both = jnp.concatenate(sums, axis=0)
    rows_sq[...] = both


def late_sums(sent, arrived):
    late = kernel(late_body, [(sent[3].shape, BF16)] * 2)
    return late(sent[3], arrived[0], sent[4], arrived[1])


def sends_of(sums, arrived, late, columns, halves):
    out = [(128, columns)] * 2 + [(64 if halves else 128, columns), (128, columns)]
    out += [(64, columns)] * halves
    return kernel(turn_body, [(s, BF16) for s in out])(sums, *arrived, *late)


def direct(blocks, move):
    _, one, two, three, *more = blocks
    return [move(one, 1), move(two, 2), move(three, -1)] + [move(m, -2) for m in more]


def joined(own, terms, columns):
    return kernel(join_body, [((128, columns), BF16)])(own, *terms)[0]


def other_replica(a):
    return lax.ppermute(a, "rep", SWAP)


def summed_over(a, move):
    return (a + move(a, -2)) + (move(a, -1) + move(a, 1))


def group_body(own, *refs):
    a, b = refs[-2:]
    a[:128] = own[...]
    a[128:] = refs[0][...]
    far = refs[1:-3]
    step = 128 // len(far)
    for k, part in enumerate(far):
        b[k * step : (k + 1) * step] = part[...]
    b[128:] = refs[-3][...]


def gathered(parts, move):
    columns = parts[0].shape[1]
    a, b = kernel(group_body, [((256, columns), BF16)] * 2)(*parts)
    next_a, next_b, last_a, last_b = move(a, -1), move(b, -1), move(a, 1), move(b, 1)
    far_a, far_b = move(next_a, -1), move(last_b, 1)
    return [a, b, next_a, next_b, far_a, far_b, last_a, last_b]


def on_device(tokens, norm_gain, w_gate, w_up, w_down, cotangent):
    zl, xi, tp = lax.axis_index("zl"), lax.axis_index("x"), lax.axis_index(TP)
    offsets = jnp.arange(16, dtype=jnp.int32)
    order = ((zl + offsets // 4) % 4) * 4 + (xi + offsets % 4) % 4
    gain_f = norm_gain.astype(F32)
    yi, ci = lax.axis_index("y"), lax.axis_index("core")
    eight = jnp.arange(8, dtype=jnp.int32)
    places = (yi + eight % 4) % 4 * 2 + (ci + eight // 4) % 2
    slots = (eight // 2 + 4 - yi) % 4 + (eight + ci) % 2 * 4

    pack_out = [(128, FIRST), (128, SECOND), (64, SECOND), (64, SECOND)]
    pack = kernel(pack_body, [(s, BF16) for s in pack_out])
    first, second, upper, lower = pack(w_gate, w_up, w_down)
    near_first = [first, over_x(first, -1), over_x(first, -2), over_x(first, 1)]
    far = [over_z(upper, -2), over_z(lower, 2)]
    near_second = [second, over_z(second, -1), *far, over_z(second, 1)]
    first = gathered(near_first, over_z)
    second = gathered(near_second, over_x)

    mine = jnp.concatenate([tokens, cotangent], axis=0)
    both = [mine, over_y(mine, -1), over_y(mine, -2), over_y(mine, 1)]
    both += [other_core(b) for b in both]
    shape, turned = ((ROWS, 2048), BF16), ((2048, ROWS), BF16)
    prepare = kernel(
        prepare_body,
        [shape, shape, turned, turned, ((ROWS, 128), F32)],
        2,
        16,
        scratch=[pltpu.VMEM((8, 2 * ROWS, 256), BF16)],
    )
    normed, dy, normed_t, dy_t, inv = prepare(order, places, *both, gain_f.reshape(8, 1, 256))
    inverse = inv[:, :1]

    out = [((ROWS, 2 * HID), BF16)]
    for columns in (FIRST, SECOND):
        out += [((n, 128, columns), BF16) for n in (4, 4, 4, 2, 2)]
    forward = kernel(
        forward_body,
        out,
        limit=16,
        scratch=[
            pltpu.VMEM((ROWS, FIRST), F32),
            pltpu.VMEM((ROWS, REST), F32),
            pltpu.VMEM((ROWS, HID), F32),
            pltpu.VMEM((ROWS, HID), BF16),
        ],
    )
    d_pair, *sent = forward(normed, dy, normed_t, dy_t, *first, *second)
    sent_first, sent_second = sent[:5], sent[5:]
    there_first = over_x(sent_first[1], 1), over_x(sent_first[2], -1)
    there_second = over_z(sent_second[1], 1), over_z(sent_second[2], -1)
    late_first = late_sums(sent_first, there_first)
    late_second = late_sums(sent_second, there_second)
    late_first = over_x(late_first[0], 1), over_x(late_first[1], -1)
    late_second = over_z(late_second[0], 1), over_z(late_second[1], -1)
    first_blocks = sends_of(sent_first[0], there_first, late_first, FIRST, True)
    second_blocks = sends_of(sent_second[0], there_second, late_second, SECOND, False)
    first_terms = direct(first_blocks, over_z)
    second_terms = direct(second_blocks, over_x)

    share = ((4, ROWS, 256), BF16)
    input_grad = kernel(
        input_grad_body, [share, share], 2, 12, scratch=[pltpu.VMEM((8, ROWS, 256), BF16)]
    )
    same, other = input_grad(order, slots, d_pair, *first, *second)
    pair_sum = kernel(pair_sum_body, [((ROWS, 256), BF16)] * 4)
    near, one, two, three = pair_sum(same, other_core(other))
    shares = near, over_y(one, 1), over_y(two, 2), over_y(three, -1)
    d_normed = sum(s.astype(F32) for s in shares)
    local_width = d_normed.shape[1]
    local_gain = lax.dynamic_slice_in_dim(gain_f, tp * local_width, local_width, 0)
    local_tokens = tokens.astype(F32)
    scaled_grad = d_normed * local_gain
    row_part = jnp.sum(scaled_grad * local_tokens, axis=-1)
    gain_part = jnp.sum(d_normed * local_tokens * inverse, axis=0, keepdims=True)
    gain_part = gain_part + other_replica(gain_part)
    first_part = joined(first_blocks[0], first_terms, FIRST)
    second_part = joined(second_blocks[0], second_terms, SECOND)
    mine_second = second_part, other_replica(second_part)
    mine_first = first_part, other_replica(first_part)
    row_part = row_part.reshape(3, 128)
    rowdot = summed_over(row_part + other_core(row_part), over_y).reshape(ROWS)
    grad_tokens = (
        cotangent.astype(F32)
        + inverse * scaled_grad
        - local_tokens * inverse**3 * rowdot[:, None] / 2048
    ).astype(BF16)
    square, wide = ((128, 128), F32), ((128, HID), F32)
    finish_second = kernel(
        finish_second_body,
        [((128, REST), F32), square, ((HID, 128), F32), ((16, 1, HID + 256), F32)],
        far=(2, 3),
    )
    up_rest, up_sq, grad_down, columns = finish_second(*mine_second, gain_part)
    arrived = to_each(columns, FS)
    down_sq, grad_gain = (jnp.sum(arrived[:, 0, at], axis=0) for at in (slice(0, HID), slice(HID, None)))
    finish_first = kernel(finish_first_body, [wide, wide, ((2, 128), F32)], far=(0, 1))
    grad_gate, grad_up, rows_sq = finish_first(*mine_first, up_rest, up_sq)
    gate_up_sq = summed_over(rows_sq + other_core(rows_sq), over_y)
    return (grad_tokens, grad_gain, grad_gate, grad_up, grad_down, gate_up_sq, down_sq)


def solution(mesh):
    fine = Mesh(mesh.devices.reshape(2, 4, 4, 4, 2), ("rep", "zl", "x", "y", "core"))
    rows = ("rep", "zl", "x")
    return jax.shard_map(
        on_device,
        mesh=fine,
        in_specs=(P(rows, TP), P(), P(FS, TP), P(FS, TP), P(TP, FS), P(rows, TP)),
        out_specs=(
            P(rows, TP),
            P(TP),
            P(FS, TP),
            P(FS, TP),
            P(TP, FS),
            P(None, FS),
            P(TP),
        ),
        check_vma=False,
    )
```
